32 devices in a mesh: sp: 4 (over z), fs: 4 (over y, x), tp: 2 (over core).
Axes of the slice: x: 2, y: 2, z: 4, core: 2. Of those that a mesh axis runs over, the one named last changes fastest.
Arguments:
- inputs: bfloat16 [4, 512, 2048], P('fs', 'sp'), may hold values from -6 to 6
- input_norm_gain: bfloat16 [2048], replicated, may hold values from 0.099609375 to 1.8984375
- receptance_matrix: bfloat16 [2048, 1024], P('fs', 'tp'), may hold values from -0.125 to 0.125
- key_matrix: bfloat16 [2048, 1024], P('fs', 'tp'), may hold values from -0.125 to 0.125
- value_matrix: bfloat16 [2048, 1024], P('fs', 'tp'), may hold values from -0.125 to 0.125
- pooling_input_weight: bfloat16 [2048, 1024], P('fs', 'tp'), may hold values from -0.125 to 0.125
- decay_lower_matrix: bfloat16 [2048, 128], replicated, may hold values from -0.125 to 0.125
- decay_raise_matrix: bfloat16 [2, 64, 1024], P(None, None, 'tp'), may hold values from -1 to 1
- decay_offset_bias: float32 [2, 1024], P(None, 'tp'), may hold values from -13 to -3
- removal_lower_matrix: bfloat16 [2048, 128], replicated, may hold values from -0.125 to 0.125
- removal_raise_matrix: bfloat16 [2, 64, 1024], P(None, None, 'tp'), may hold values from -1 to 1
- removal_rate_bias: float32 [2, 1024], P(None, 'tp'), may hold values from -9 to 1.5
- tempo_scale: float32 [4, 2, 16, 512], P('fs', None, 'tp', 'sp'), may hold values from 0.3 to 3.2, as said below
- sudden_decay_extra: float32 [4, 2, 16, 512], P('fs', None, 'tp', 'sp'), may hold values from -2.8 to 0
- head_norm_gain: bfloat16 [1024], P('tp'), may hold values from 0.099609375 to 1.8984375
- group_mixing_weight: bfloat16 [4, 256, 256], P('tp'), may hold values from -0.375 to 0.375
- attention_output_matrix: bfloat16 [2048, 1024], P('fs', 'tp'), may hold values from -0.125 to 0.125
- pooling_output_matrix: bfloat16 [2048, 1024], P('fs', 'tp'), may hold values from -0.125 to 0.125
Outputs:
- mixed_out: bfloat16 [4, 512, 2048], P('fs', ('sp', 'tp'))
The draws below stay inside these ranges and needn't reach their ends.
Inputs may be any that keep to these rules, and one draw needn't show every extreme that they name: `tempo_scale`: positive.
All inputs are finite; a program needn't handle non-finite values.
Results may differ from the reference program's by a relative error of at most 0.017.
Values may be sent and summed in bfloat16 or wider, within the bound.
A program may use at most 128 MiB of HBM per device.

```python
import math
import jax
import jax.numpy as jnp
from jax import lax

D = 2048
HEADS_A = 16
HEAD = 64
DECAY_RANK = 64
RATE_RANK = 64
POOL_GROUPS = 4
GROUP_WIDTH = 256
T_DEV = 128
D_A = 1024
D_POOL = 1024
LEN = 512
SEQS = 4
N_SP = 4


def slow_mask(key):
    marks = []
    for travel_direction in range(2):
        order = jax.random.permutation(jax.random.fold_in(key, 41 + travel_direction), HEADS_A)
        marks.append((order < HEADS_A // 2).astype(jnp.float32))
    return jnp.repeat(jnp.stack(marks, axis=0), HEAD, axis=1)


def draw_decay_offset_bias(key, part):
    slow = slow_mask(key)
    jitter = jax.random.uniform(jax.random.fold_in(key, 5), (2, HEADS_A * HEAD), jnp.float32, -0.5, 0.5)
    slow_level = jnp.log(1.0 / (6.0 * LEN)) + 0.1
    fast_level = math.log(1.0 / 60.0) + 0.5
    return slow * slow_level + (1.0 - slow) * fast_level + jitter


def draw_removal_rate_bias(key, part):
    slow = slow_mask(key)
    jitter = jax.random.uniform(jax.random.fold_in(key, 6), (2, HEADS_A * HEAD), jnp.float32, -0.5, 0.5)
    fast_vals = jax.random.uniform(jax.random.fold_in(key, 7), (2, HEADS_A * HEAD), jnp.float32, -1.5, 1.5)
    return slow * (jnp.log(8.0 / LEN) + jitter) + (1.0 - slow) * fast_vals


def draw_tempo_scale(key, part):
    low, high = (0.5, 2.0)
    factor = jnp.exp(jax.random.uniform(jax.random.fold_in(key, 21), (SEQS, 2, HEADS_A, N_SP), jnp.float32, math.log(low), math.log(high)))
    factor = jnp.repeat(factor, T_DEV, axis=3)
    jitter = jax.random.uniform(jax.random.fold_in(key, 22), (SEQS, 2, HEADS_A, LEN), jnp.float32, 0.8, 1.25)
    return factor * jitter


def draw_sudden_decay_extra(key, part):
    places = jax.random.randint(jax.random.fold_in(key, 31), (SEQS, 2, HEADS_A, 4), 0, LEN)
    kept = jax.random.uniform(jax.random.fold_in(key, 32), (SEQS, 2, HEADS_A, 4), jnp.float32, 0.5, 0.8)
    lost = jnp.log(kept)
    spots = jnp.arange(LEN)
    marked = jnp.where(spots[None, None, None, None, :] == places[..., None], lost[..., None], 0.0)
    return jnp.sum(marked, axis=3).astype(jnp.float32)


def levels(stream_key, shape, shards, smallest, high):
    def one(axis_at, blocks):
        heights = jax.random.uniform(jax.random.fold_in(jax.random.fold_in(stream_key, 6), axis_at), (blocks,), jnp.float32, smallest / len(shards), high / len(shards))
        return jnp.repeat(jnp.exp(heights), shape[axis_at] // blocks).reshape((-1,) + (1,) * (len(shape) - axis_at - 1))

    factor_of = one(*shards[0])
    for cut in shards[1:]:
        factor_of = factor_of * one(*cut)
    return factor_of


def scatter_about(key, shape, deviation, most, pieces=(), dtype=jnp.bfloat16):
    drawn = deviation * jax.random.normal(key, shape, jnp.float32)
    if pieces:
        drawn = drawn * levels(key, shape, pieces, -0.22, 0.18)
    return jnp.clip(drawn, -most, most).astype(dtype)


def setup_inputs(seed: int = 0) -> dict:
    keys = jax.random.split(jax.random.key(seed), 19)
    inputs = scatter_about(keys[0], (SEQS, LEN, D), 1.0, 6.0, ((0, 4), (1, 4)))
    input_norm_gain = jnp.clip(1.0 + 0.18 * jax.random.normal(keys[1], (D,), jnp.float32), 0.099609375, 1.8984375).astype(jnp.bfloat16)
    receptance_matrix = scatter_about(keys[2], (D, D_A), D ** -0.5, 0.125, ((0, 4), (1, 2)))
    key_matrix = scatter_about(keys[3], (D, D_A), D ** -0.5, 0.125, ((0, 4), (1, 2)))
    value_matrix = scatter_about(keys[4], (D, D_A), D ** -0.5, 0.125, ((0, 4), (1, 2)))
    pooling_input_weight = scatter_about(keys[5], (D, D_POOL), D ** -0.5, 0.125, ((0, 4), (1, 2)))
    decay_lower_matrix = scatter_about(keys[6], (D, 2 * DECAY_RANK), D ** -0.5, 0.125)
    decay_raise_matrix = scatter_about(keys[7], (2, DECAY_RANK, D_A), (DECAY_RANK // 2) ** -0.5, 1.0, ((2, 2),))
    decay_offset_bias = draw_decay_offset_bias(jax.random.fold_in(keys[18], 71), 0)
    removal_lower_matrix = scatter_about(keys[9], (D, 2 * RATE_RANK), D ** -0.5, 0.125)
    removal_raise_matrix = scatter_about(keys[10], (2, RATE_RANK, D_A), (RATE_RANK // 2) ** -0.5, 1.0, ((2, 2),))
    removal_rate_bias = draw_removal_rate_bias(jax.random.fold_in(keys[18], 71), 0)
    tempo_scale = draw_tempo_scale(jax.random.fold_in(keys[18], 71), 0)
    sudden_decay_extra = draw_sudden_decay_extra(jax.random.fold_in(keys[18], 71), 0)
    head_norm_gain = jnp.clip(1.0 + 0.18 * jax.random.normal(keys[14], (D_A,), jnp.float32), 0.099609375, 1.8984375).astype(jnp.bfloat16)
    group_mixing_weight = scatter_about(keys[15], (POOL_GROUPS, GROUP_WIDTH, GROUP_WIDTH), GROUP_WIDTH ** -0.5, 0.375, ((0, 2),))
    attention_output_matrix = scatter_about(keys[16], (D, D_A), (D_A + D_POOL) ** -0.5, 0.125, ((0, 4), (1, 2)))
    pooling_output_matrix = scatter_about(keys[17], (D, D_POOL), (D_A + D_POOL) ** -0.5, 0.125, ((0, 4), (1, 2)))
    return dict(inputs=inputs, input_norm_gain=input_norm_gain, receptance_matrix=receptance_matrix, key_matrix=key_matrix, value_matrix=value_matrix, pooling_input_weight=pooling_input_weight, decay_lower_matrix=decay_lower_matrix, decay_raise_matrix=decay_raise_matrix, decay_offset_bias=decay_offset_bias, removal_lower_matrix=removal_lower_matrix, removal_raise_matrix=removal_raise_matrix, removal_rate_bias=removal_rate_bias, tempo_scale=tempo_scale, sudden_decay_extra=sudden_decay_extra, head_norm_gain=head_norm_gain, group_mixing_weight=group_mixing_weight, attention_output_matrix=attention_output_matrix, pooling_output_matrix=pooling_output_matrix)


norm_eps = 1e-06
head_eps = 0.00064
unit_eps = 1e-06
highest = lax.Precision.HIGHEST

def project(left, weight):
    return jnp.dot(left, weight, preferred_element_type=jnp.float32).astype(jnp.bfloat16)

def window_diff(values, half):
    running = jnp.concatenate([jnp.zeros((1, values.shape[1]), jnp.float32), jnp.cumsum(values, axis=0)], axis=0)
    spots = jnp.arange(LEN)
    upper = jnp.minimum(spots + half, LEN)
    lower = jnp.maximum(spots - half, 0)
    counts = (upper - lower).astype(jnp.float32)
    return (running[upper] - running[lower]) / counts[:, None] - values

def recur(state, element_list):
    decay, unit, removal, written, value, recept = element_list
    pulled = jnp.einsum('hvk,hk->hv', state, unit, precision=highest)
    state = state * jnp.exp(decay)[:, None, :] - pulled[:, :, None] * removal[:, None, :] + value[:, :, None] * written[:, None, :]
    return (state, jnp.einsum('hvk,hk->hv', state, recept, precision=highest))

def reference(inputs, input_norm_gain, receptance_matrix, key_matrix, value_matrix, pooling_input_weight, decay_lower_matrix, decay_raise_matrix, decay_offset_bias, removal_lower_matrix, removal_raise_matrix, removal_rate_bias, tempo_scale, sudden_decay_extra, head_norm_gain, group_mixing_weight, attention_output_matrix, pooling_output_matrix):

    def single_sequence(element_list):
        row_block, decay_tempo, sudden_jump = element_list
        values = row_block.astype(jnp.float32)
        normed = (values * lax.rsqrt(lax.optimization_barrier(jnp.mean(values * values, axis=-1, keepdims=True)) + norm_eps) * input_norm_gain.astype(jnp.float32)).astype(jnp.bfloat16)
        receptance = project(normed, receptance_matrix).astype(jnp.float32).reshape(LEN, HEADS_A, HEAD)
        key_rows = project(normed, key_matrix).astype(jnp.float32).reshape(LEN, HEADS_A, HEAD)
        val_rows = project(normed, value_matrix).astype(jnp.float32).reshape(LEN, HEADS_A, HEAD)
        pool_in = project(normed, pooling_input_weight).astype(jnp.float32)
        decay_act = jnp.tanh(project(normed, decay_lower_matrix).astype(jnp.float32)).astype(jnp.bfloat16)
        rate_latent = project(normed, removal_lower_matrix)
        unit_keys = key_rows * lax.rsqrt(lax.optimization_barrier(jnp.sum(key_rows * key_rows, axis=-1, keepdims=True)) + unit_eps)
        readout = jnp.zeros((LEN, HEADS_A, HEAD), jnp.float32)
        for travel_direction in range(2):
            part = decay_act[:, travel_direction * DECAY_RANK:(travel_direction + 1) * DECAY_RANK]
            decay_pre = decay_offset_bias[travel_direction] + jnp.dot(part, decay_raise_matrix[travel_direction], preferred_element_type=jnp.float32)
            decay_velocity = jnp.exp(-jax.nn.softplus(-decay_pre) - 0.5).reshape(LEN, HEADS_A, HEAD)
            logarithm_decay = -decay_velocity * decay_tempo[travel_direction].T[:, :, None] + sudden_jump[travel_direction].T[:, :, None]
            latent = rate_latent[:, travel_direction * RATE_RANK:(travel_direction + 1) * RATE_RANK]
            rate = jax.nn.sigmoid(removal_rate_bias[travel_direction] + jnp.dot(latent, removal_raise_matrix[travel_direction], preferred_element_type=jnp.float32))
            rate = rate.reshape(LEN, HEADS_A, HEAD)
            start = jnp.zeros((HEADS_A, HEAD, HEAD), jnp.float32)
            _, reads = lax.scan(recur, start, (logarithm_decay, unit_keys, unit_keys * rate, key_rows * rate, val_rows, receptance), reverse=travel_direction == 1)
            readout = readout + reads
        centred = readout - lax.optimization_barrier(jnp.mean(readout, axis=-1, keepdims=True))
        spread = lax.optimization_barrier(jnp.mean(centred * centred, axis=-1, keepdims=True))
        attn_out = (centred * lax.rsqrt(spread + head_eps)).reshape(LEN, HEADS_A * HEAD) * head_norm_gain.astype(jnp.float32)
        attn_out = attn_out.astype(jnp.bfloat16)
        diffs = [window_diff(pool_in[:, group * GROUP_WIDTH:(group + 1) * GROUP_WIDTH], 2 ** group) for group in range(POOL_GROUPS)]
        pool_diff = jnp.concatenate(diffs, axis=1).astype(jnp.bfloat16)
        mixed = [jnp.dot(pool_diff[:, group * GROUP_WIDTH:(group + 1) * GROUP_WIDTH], group_mixing_weight[group], preferred_element_type=jnp.float32) for group in range(POOL_GROUPS)]
        pool_out = jnp.concatenate(mixed, axis=1).astype(jnp.bfloat16)
        merged = jnp.dot(attn_out, attention_output_matrix.T, preferred_element_type=jnp.float32) + jnp.dot(pool_out, pooling_output_matrix.T, preferred_element_type=jnp.float32)
        return merged.astype(jnp.bfloat16)
    return lax.map(single_sequence, (inputs, tempo_scale, sudden_decay_extra))
```

```python
import functools

import jax
import jax.numpy as jnp
from jax import lax
from jax.experimental import pallas as pl
from jax.experimental.pallas import tpu as pltpu
from jax.sharding import PartitionSpec as P

HEAD = 64
GROUP_WIDTH = 256
LANES = 128
BLOCK = 16
HALO = 16
PER = 2

norm_eps = 1e-06
head_eps = 0.00064
unit_eps = 1e-06
f32 = jnp.float32
bf16 = jnp.bfloat16
VMEM = pl.BlockSpec(memory_space=pltpu.VMEM)


def dot(left, right):
    return jnp.dot(left.astype(bf16), right.astype(bf16), preferred_element_type=f32)


def dot_general(left, right, dims):
    return lax.dot_general(
        left.astype(bf16), right.astype(bf16), (dims, ((), ())), preferred_element_type=f32
    )


def dot_rows(left, right):
    return dot_general(left, right, ((1,), (1,)))


def dot_cols(left, right):
    return dot_general(left, right, ((0,), (0,)))


def split_exact(cells, pieces):
    parts = []
    for _ in range(pieces - 1):
        high = cells.astype(bf16).astype(f32)
        parts.append(high)
        cells = cells - high
    return parts + [cells]


def remote(src, dst, send, recv, axis, peer):
    return pltpu.make_async_remote_copy(
        src_ref=src,
        dst_ref=dst,
        send_sem=send,
        recv_sem=recv,
        device_id={axis: peer},
        device_id_type=pl.DeviceIdType.MESH,
    )


def greet(barrier, axis, peer):
    pl.semaphore_signal(
        barrier, inc=1, device_id={axis: peer}, device_id_type=pl.DeviceIdType.MESH
    )


def flipped(at, bits):
    moved = at
    bit = 1
    while bit <= bits:
        if bits & bit:
            moved = moved + bit - 2 * bit * lax.rem(at // bit, 2)
        bit *= 2
    return moved


def front_part(
    n,
    x_ref,
    gain_ref,
    weights,
    lowers,
    loads,
    pool_ref,
    lat_ref,
    mine,
    cells,
    part,
    pool_part,
    onward,
    pool_onward,
    landed,
    pool_landed,
    joined,
    pool_joined,
    xs,
    xr,
    ps,
    pr,
    qs,
    qr,
    count,
    mix_group,
):
    me = lax.axis_index("fs")
    core, ntp = lax.axis_index("tp"), lax.axis_size("tp")
    width = x_ref.shape[2] // n
    share = x_ref.shape[1] // ntp
    rows = pl.ds(pl.multiple_of(core * share, share), share)
    groups = part.shape[0]
    wide = part.shape[4]
    x = x_ref[0].astype(f32)
    with jax.named_scope("norm"):
        normed = (
            x
            * lax.rsqrt(jnp.mean(x * x, axis=-1, keepdims=True) + norm_eps)
            * gain_ref[...].astype(f32).reshape(1, -1)
        ).astype(bf16)
        for j in range(n):
            mine[j] = normed[:, j * width : (j + 1) * width]
    with jax.named_scope("barrier"):
        pl.semaphore_wait(pltpu.get_barrier_semaphore(), count)
    order = list(range(n - 1, 0, -1))
    moves = []
    for d in order:
        peer = flipped(me, d)
        copy = remote(
            mine.at[peer, rows], cells.at[me, rows], xs.at[d, 0], xr.at[d, 0], "fs", peer
        )
        copy.start()
        moves.append(copy)
    with jax.named_scope("latent"):
        for load in loads[:2]:
            load.wait()
        dl_ref, rl_ref = lowers
        decay = jnp.zeros((x.shape[0], dl_ref.shape[1]), f32)
        rate = jnp.zeros((x.shape[0], rl_ref.shape[1]), f32)
        for j in range(n):
            block = mine[j]
            decay = decay + dot(block, dl_ref[j * width : (j + 1) * width])
            rate = rate + dot(block, rl_ref[j * width : (j + 1) * width])
        lat_ref[0] = jnp.tanh(decay.astype(bf16).astype(f32)).astype(bf16)
        lat_ref[1] = rate.astype(bf16)
        for load in loads[2:]:
            load.wait()
    with jax.named_scope("xwait"):
        for d, copy in zip(order, list(moves)):
            peer = flipped(me, d)
            copy.wait_recv()
            for e in range(1, ntp):
                passed = remote(
                    cells.at[peer, rows],
                    cells.at[peer, rows],
                    xs.at[d, e],
                    xr.at[d, e],
                    "tp",
                    lax.rem(core + e, ntp),
                )
                passed.start()
                moves.append(passed)
        for copy in moves[len(order) :]:
            copy.wait_recv()

    first, second, across = routes(me, n, core)
    targets = (first, across)

    def first_copy(g, slot):
        return remote(
            part.at[g, slot], landed.at[g, slot], ps.at[g, slot], pr.at[g, slot], "fs", first
        )

    def first_pool(slot):
        return remote(
            pool_part.at[slot],
            pool_landed.at[slot],
            ps.at[groups, slot],
            pr.at[groups, slot],
            "fs",
            first,
        )

    def second_copy(g):
        return remote(onward.at[g], joined.at[g], qs.at[g], qr.at[g], "fs", second)

    second_pool = remote(
        pool_onward, pool_joined, qs.at[groups], qr.at[groups], "fs", second
    )

    def piece(m, g):
        return weights[m][:, g * wide : (g + 1) * wide]

    with jax.named_scope("partials"):
        for g in range(groups):
            for slot in (1, 0):
                for m in range(3):
                    part[g, slot, m] = dot(cells[targets[slot]], piece(m, g)).astype(bf16)
                first_copy(g, slot).start()
        for slot in (1, 0):
            pool_part[slot] = dot(cells[targets[slot]], weights[3][...]).astype(bf16)
            first_pool(slot).start()

    def forward(g):
        with jax.named_scope(f"fwd{g}"):
            first_copy(g, 1).wait_recv()
            for m in range(3):
                onward[g, m] = (
                    dot(cells[second], piece(m, g)) + landed[g, 1, m].astype(f32)
                ).astype(bf16)
            second_copy(g).start()

    def forward_pool():
        with jax.named_scope("fwdpool"):
            first_pool(1).wait_recv()
            pool_onward[...] = (
                dot(cells[second], weights[3][...]) + pool_landed[1].astype(f32)
            ).astype(bf16)
            second_pool.start()

    def settle(g):
        with jax.named_scope(f"settle{g}"):
            first_copy(g, 0).wait_recv()
            second_copy(g).wait_recv()
        with jax.named_scope(f"mix{g}"):
            owned = [
                (
                    dot(mine[me], piece(m, g))
                    + landed[g, 0, m].astype(f32)
                    + joined[g, m].astype(f32)
                ).astype(bf16)
                for m in range(3)
            ]
            mix_group(g, *owned)

    for g in range(groups):
        forward(g)
    for g in range(groups):
        settle(g)
        if g == 0:
            forward_pool()
    with jax.named_scope("poolin"):
        first_pool(0).wait_recv()
        second_pool.wait_recv()
        pool_ref[...] = (
            dot(mine[me], weights[3][...])
            + pool_landed[0].astype(f32)
            + pool_joined[...].astype(f32)
        ).astype(bf16)

    def finish():
        for copy in moves:
            copy.wait_send()
        for g in range(groups):
            for slot in (1, 0):
                first_copy(g, slot).wait_send()
            second_copy(g).wait_send()
        for slot in (1, 0):
            first_pool(slot).wait_send()
        second_pool.wait_send()

    return finish


def routes(me, n, core):
    low, high = flipped(me, 1), flipped(me, n // 2)
    odd = lax.rem(core, 2)
    return low + odd * (high - low), high + odd * (low - high), flipped(me, n // 2 + 1)


def mix_group(
    g,
    key,
    receptance,
    value,
    lat_ref,
    draise_ref,
    dbias_ref,
    rraise_ref,
    rbias_ref,
    tempo_ref,
    extra_ref,
    query_ref,
    local_ref,
    transfer_ref,
    carried_ref,
):
    tokens, wide = key.shape
    per = wide // LANES
    lanes = slice(g * wide, (g + 1) * wide)
    kf = key.astype(f32)
    rf = receptance.astype(f32)
    lane = lax.broadcasted_iota(jnp.int32, (tokens, LANES), 1)
    row = lax.broadcasted_iota(jnp.int32, (tokens, LANES), 0)
    head0 = lane < HEAD
    only = [head0.astype(f32).astype(bf16), (~head0).astype(f32).astype(bf16)]
    blank = jnp.zeros((tokens, LANES), bf16)

    def cut(cells, j):
        return cells[:, j * LANES : (j + 1) * LANES]

    def both_heads(cells):
        return jnp.concatenate([cells * only[0], cells * only[1]], 0)

    def rows_for_heads(cells):
        return jnp.concatenate(
            [jnp.concatenate([cut(cells, i) * o for i in range(cells.shape[1] // LANES)], 1) for o in only], 0
        )

    units = []
    for j in range(per):
        kj = cut(kf, j)
        k2 = kj * kj
        s0 = jnp.sum(jnp.where(head0, k2, 0.0), axis=-1, keepdims=True)
        s1 = jnp.sum(jnp.where(head0, 0.0, k2), axis=-1, keepdims=True)
        units.append(kj * lax.rsqrt(jnp.where(head0, s0, s1) + unit_eps))
    heads = tempo_ref.shape[1]
    spread = (
        lax.broadcasted_iota(jnp.int32, (heads, wide), 0)
        == 2 * per * g + lax.broadcasted_iota(jnp.int32, (heads, wide), 1) // HEAD
    ).astype(f32)
    spread = jnp.concatenate([spread] * 3, 0)

    def spread_out(cells):
        return dot_cols(jnp.concatenate(split_exact(cells, 3), 0), spread)

    blocks = tokens // BLOCK
    zero_row = jnp.zeros((1, LANES), f32)
    eye = (row == lane).astype(f32)
    sizes = []
    size = 1
    while size < tokens:
        sizes.append(size)
        size *= 2

    def level_mask(k):
        return ((row >> (k + 1)) == (lane >> (k + 1))) & ((row >> k) != (lane >> k))

    ways = [[] for _ in range(per)]
    for d in range(2):
        lat_mask = head0 if d == 0 else ~head0
        lat_d = jnp.where(lat_mask, lat_ref[0].astype(f32), 0.0)
        lat_r = jnp.where(lat_mask, lat_ref[1].astype(f32), 0.0)
        pre = dbias_ref[d : d + 1, lanes] + dot(lat_d, draise_ref[:, lanes])
        velocity = jax.nn.sigmoid(pre) * 0.6065306597126334
        ld = -velocity * spread_out(tempo_ref[d]) + spread_out(extra_ref[d])
        rates = jax.nn.sigmoid(rbias_ref[d : d + 1, lanes] + dot(lat_r, rraise_ref[:, lanes]))
        upto = (lane <= row) if d == 0 else (lane >= row)
        strict = (lane < row) if d == 0 else (lane > row)
        tri = upto.astype(f32).astype(bf16)
        inners = dot(
            jnp.concatenate([tri, tri], 1), jnp.concatenate(split_exact(ld, 2), 0)
        )
        for j in range(per):
            inner = cut(inners, j)
            excl = inner - cut(ld, j)
            unit, query_in = units[j], cut(rf, j)
            removal = unit * cut(rates, j)
            written = cut(kf, j) * cut(rates, j)
            grams = []
            for i in range(blocks):
                lo, hi = i * BLOCK, (i + 1) * BLOCK
                if d == 0:
                    base = inner[lo - 1 : lo] if i > 0 else zero_row
                    live = slice(0, hi)
                else:
                    base = inner[hi : hi + 1] if i < blocks - 1 else zero_row
                    live = slice(lo, tokens)
                ahead = unit[lo:hi] * jnp.exp(excl[lo:hi] - base)
                query = query_in[lo:hi] * jnp.exp(inner[lo:hi] - base)
                grow = jnp.exp(jnp.minimum(base - inner[live], 80.0))
                rest = tokens - grow.shape[0]

                def filled(cells):
                    cells = cells.astype(bf16)
                    if not rest:
                        return cells
                    empty = jnp.zeros((rest, LANES), bf16)
                    return jnp.concatenate([cells, empty] if d == 0 else [empty, cells], 0)

                right = jnp.concatenate(
                    [filled(removal[live] * grow), filled(written[live] * grow)], 0
                )
                h0 = head0[lo:hi]
                left = jnp.concatenate(
                    [
                        jnp.where(h0, ahead, 0.0),
                        jnp.where(h0, 0.0, ahead),
                        jnp.where(h0, query, 0.0),
                        jnp.where(h0, 0.0, query),
                    ],
                    0,
                )
                grams.append(dot_rows(left, right))

            def gathered(place, at, mask):
                rows = jnp.concatenate(
                    [
                        gram[place * BLOCK : (place + 1) * BLOCK, at * tokens : (at + 1) * tokens]
                        for gram in grams
                    ],
                    0,
                )
                return jnp.where(mask, rows, 0.0)

            way = dict(inner=inner, excl=excl, removal=removal, written=written)
            way["link"] = [gathered(h, 0, strict) for h in range(2)]
            way["write"] = [gathered(h, 1, strict).astype(bf16) for h in range(2)]
            way["read"] = [gathered(2 + h, 0, upto).astype(bf16) for h in range(2)]
            way["read_write"] = [gathered(2 + h, 1, upto).astype(bf16) for h in range(2)]
            ways[j].append(way)

    links = [link for j in range(per) for way in ways[j] for link in way["link"]]
    mask = level_mask(0)
    inverses = [(eye - jnp.where(mask, a, 0.0)).astype(bf16) for a in links]
    links = [a.astype(bf16) for a in links]

    def products(lefts, rights):
        out = []
        for i in range(0, len(lefts), 2):
            result = dot(
                jnp.concatenate(lefts[i : i + 2], 1),
                jnp.concatenate(
                    [
                        jnp.concatenate([rights[i], blank], 1),
                        jnp.concatenate([blank, rights[i + 1]], 1),
                    ],
                    0,
                ),
            ).astype(bf16)
            out += [cut(result, 0), cut(result, 1)]
        return out

    for k in range(1, len(sizes)):
        mask = level_mask(k).astype(f32).astype(bf16)
        firsts = products(inverses, [a * mask for a in links])
        steps = products(firsts, inverses)
        inverses = [t - u for t, u in zip(inverses, steps)]

    block_diag = (row < HEAD) == head0
    for j in range(per):
        pair = g * per + j
        vj = cut(value, j)
        stacked = both_heads(vj)
        sums = dot(
            jnp.concatenate(
                [
                    jnp.concatenate(way[name], 1)
                    for way in ways[j]
                    for name in ("write", "read_write")
                ],
                0,
            ),
            stacked,
        )
        local = sums[tokens : 2 * tokens] + sums[3 * tokens :]
        for d, way in enumerate(ways[j]):
            inner, excl = way["inner"], way["excl"]
            last = inner[tokens - 1 : tokens] if d == 0 else inner[0:1]
            ahead = units[j] * jnp.exp(excl)
            query = cut(rf, j) * jnp.exp(inner)
            tail = jnp.exp(last - inner)
            base = sums[2 * d * tokens : (2 * d + 1) * tokens]
            rhs = jnp.concatenate([ahead.astype(bf16), base.astype(bf16)], 1)
            at = 4 * j + 2 * d
            solved = -dot(jnp.concatenate(inverses[at : at + 2], 1), rows_for_heads(rhs))
            solved = solved.astype(bf16)
            pull_map, pull_base = cut(solved, 0), cut(solved, 1)
            remove_tail = (way["removal"] * tail).astype(bf16)
            write_tail = (way["written"] * tail).astype(bf16)
            seen = dot(jnp.concatenate(way["read"], 1), rows_for_heads(solved))
            query_ref[d, :, pair * LANES : (pair + 1) * LANES] = (query + cut(seen, 0)).astype(bf16)
            local = local + cut(seen, 1)
            transfer = (
                jnp.where(block_diag, dot_cols(pull_map, remove_tail), 0.0) + eye * jnp.exp(last)
            )
            transfer_ref[d, pair] = transfer.astype(bf16)
            carried = dot_cols(
                jnp.concatenate([pull_base, vj], 0),
                jnp.concatenate([remove_tail, write_tail], 0),
            )
            carried = jnp.where(block_diag, carried, 0.0)
            carried_ref[d, pair] = carried[:HEAD] + carried[HEAD:]
        local_ref[:, pair * LANES : (pair + 1) * LANES] = local


def layer_kernel(
    nsp,
    nfs,
    ntp,
    x_ref,
    in_gain_ref,
    wk_hbm,
    wr_hbm,
    wv_hbm,
    wi_hbm,
    dl_hbm,
    rl_hbm,
    draise_ref,
    dbias_ref,
    rraise_ref,
    rbias_ref,
    tempo_ref,
    extra_ref,
    mix_hbm,
    gain_ref,
    wa_hbm,
    wp_hbm,
    out_ref,
    wk_ref,
    wr_ref,
    wv_ref,
    wi_ref,
    dl_ref,
    rl_ref,
    mix_ref,
    wa_ref,
    wp_ref,
    loaded,
    mine,
    cells,
    part,
    pool_part,
    onward,
    pool_onward,
    landed,
    pool_landed,
    joined,
    pool_joined,
    xs,
    xr,
    ps,
    pr,
    qs,
    qr,
    lat_ref,
    pool_ref,
    query_ref,
    local_ref,
    transfer_ref,
    carried_ref,
    edge,
    halo,
    incoming,
    leaving,
    act,
    tsend,
    trecv,
    sums_ref,
    osend,
    orecv,
    hs,
    hr,
    ss,
    sr,
    gs,
    gr,
    ts,
    tr,
    os,
    orr,
):
    z = lax.axis_index("sp")
    me = lax.axis_index("fs")
    core = lax.axis_index("tp")
    tokens, channels = local_ref.shape
    half_rows = tokens // ntp
    has_prev = z > 0
    has_next = z < nsp - 1
    prev = jnp.maximum(z - 1, 0)
    after = jnp.minimum(z + 1, nsp - 1)

    barrier = pltpu.get_barrier_semaphore()
    for d in range(1, nfs):
        greet(barrier, "fs", flipped(me, d))
    for d in range(1, ntp):
        greet(barrier, "tp", lax.rem(core + d, ntp))
    pl.when(has_prev)(lambda: greet(barrier, "sp", prev))
    pl.when(has_next)(lambda: greet(barrier, "sp", after))
    count = nfs + ntp - 2 + jnp.where(has_prev, 1, 0) + jnp.where(has_next, 1, 0)
    sources = (dl_hbm, rl_hbm, wk_hbm, wr_hbm, wv_hbm, wi_hbm, mix_hbm, wa_hbm, wp_hbm)
    targets = (dl_ref, rl_ref, wk_ref, wr_ref, wv_ref, wi_ref, mix_ref, wa_ref, wp_ref)
    loads = [
        pltpu.make_async_copy(source, target, loaded.at[i])
        for i, (source, target) in enumerate(zip(sources, targets))
    ]
    for load in loads:
        load.start()
    def state_copy(d, g):
        return remote(
            leaving.at[d, g],
            incoming.at[d, g],
            ss.at[d, g],
            sr.at[d, g],
            "sp",
            after if d == 0 else prev,
        )

    halo_copies = [
        remote(edge.at[1], halo.at[0], hs.at[0], hr.at[0], "sp", after),
        remote(edge.at[0], halo.at[1], hs.at[1], hr.at[1], "sp", prev),
    ]
    sends = [has_next, has_prev]
    takes = [has_prev, has_next]
    groups = incoming.shape[1]
    per = incoming.shape[2]

    def mix_step(g, *operands):
        mix_group(g, *operands)
        for d in range(2):

            @pl.when(jnp.logical_not(takes[d]))
            def _():
                incoming[d, g] = jnp.zeros_like(incoming[d, g])
                for j in range(per):
                    leaving[d, g, j] = carried_ref[d, g * per + j].astype(bf16)
                pl.when(sends[d])(lambda: state_copy(d, g).start())

    def relay(d, g):
        @pl.when(takes[d])
        def _():
            state_copy(d, g).wait_recv()

            @pl.when(sends[d])
            def _():
                for j in range(per):
                    p = g * per + j
                    leaving[d, g, j] = (
                        dot(incoming[d, g, j], transfer_ref[d, p]) + carried_ref[d, p]
                    ).astype(bf16)
                state_copy(d, g).start()

    early = 2 * z < nsp

    def relays(near, g):
        @pl.when(early)
        def _():
            relay(0 if near else 1, g)

        @pl.when(jnp.logical_not(early))
        def _():
            relay(1 if near else 0, g)

    finish_front = front_part(
        nfs,
        x_ref,
        in_gain_ref,
        (wk_ref, wr_ref, wv_ref, wi_ref),
        (dl_ref, rl_ref),
        loads[:6],
        pool_ref,
        lat_ref,
        mine,
        cells,
        part,
        pool_part,
        onward,
        pool_onward,
        landed,
        pool_landed,
        joined,
        pool_joined,
        xs,
        xr,
        ps,
        pr,
        qs,
        qr,
        count,
        lambda g, key, receptance, value: mix_step(
            g,
            key,
            receptance,
            value,
            lat_ref,
            draise_ref,
            dbias_ref,
            rraise_ref,
            rbias_ref,
            tempo_ref,
            extra_ref,
            query_ref,
            local_ref,
            transfer_ref,
            carried_ref,
        ),
    )
    for load in loads[6:]:
        load.wait()
    with jax.named_scope("relayA0"):
        relays(True, 0)
    edge[0] = pool_ref[:HALO]
    edge[1] = pool_ref[tokens - HALO :]
    for d in range(2):
        pl.when(sends[d])(lambda: halo_copies[d].start())
    for g in range(1, groups):
        with jax.named_scope(f"relayA{g}"):
            relays(True, g)
    with jax.named_scope("halo"):
        for d in range(2):

            @pl.when(takes[d])
            def _():
                halo_copies[d].wait_recv()

            @pl.when(jnp.logical_not(takes[d]))
            def _():
                halo[d] = jnp.zeros_like(halo[d])

    span = tokens + 2 * HALO
    rim = jnp.concatenate([halo[0], pool_ref[...], halo[1]], 0)
    here = lax.broadcasted_iota(jnp.int32, (tokens, span), 0)
    there = lax.broadcasted_iota(jnp.int32, (tokens, span), 1) - HALO
    position = z * tokens + lax.broadcasted_iota(jnp.int32, (tokens, GROUP_WIDTH), 0)
    length = tokens * nsp
    groups_here = channels // GROUP_WIDTH
    for member in range(groups_here):
        cols = slice(member * GROUP_WIDTH, (member + 1) * GROUP_WIDTH)
        reach = jnp.left_shift(1, core * groups_here + member)
        window = jnp.where((there >= here - reach) & (there < here + reach), 1.0, 0.0)
        total = dot(window, rim[:, cols])
        size = (
            jnp.minimum(position + reach, length) - jnp.maximum(position - reach, 0)
        ).astype(f32)
        diff = (total / size - pool_ref[:, cols].astype(f32)).astype(bf16)
        act[me, 0, :, cols] = dot(diff, mix_ref[member]).astype(bf16)
    order = list(range(nfs - 1, 0, -1))
    shares = []
    for d in order:
        peer = flipped(me, d)
        copy = remote(act.at[me, 0], act.at[me, 0], gs.at[d, 0], gr.at[d, 0], "fs", peer)
        copy.start()
        shares.append(copy)

    head0 = lax.broadcasted_iota(jnp.int32, (tokens, LANES), 1) < HEAD
    top0 = lax.broadcasted_iota(jnp.int32, (HEAD, LANES), 1) < HEAD

    def head_mean(values):
        low = jnp.sum(jnp.where(head0, values, 0.0), axis=-1, keepdims=True)
        high = jnp.sum(jnp.where(head0, 0.0, values), axis=-1, keepdims=True)
        return jnp.where(head0, low, high) * (1.0 / HEAD)

    for g in range(groups):
        with jax.named_scope(f"relayB{g}"):
            relays(False, g)
        with jax.named_scope(f"readout{g}"):
            for j in range(per):
                p = g * per + j
                lanes = slice(p * LANES, (p + 1) * LANES)
                readout = local_ref[:, lanes]
                for d in range(2):
                    state = incoming[d, g, j].astype(f32)
                    whole = jnp.concatenate(
                        [jnp.where(top0, state, 0.0), jnp.where(top0, 0.0, state)], 0
                    )
                    readout = readout + dot_rows(query_ref[d, :, lanes], whole)
                centred = readout - head_mean(readout)
                scaled = centred * lax.rsqrt(head_mean(centred * centred) + head_eps)
                act[me, 1, :, lanes] = (
                    scaled * gain_ref[lanes].astype(f32).reshape(1, -1)
                ).astype(bf16)
            cols = pl.ds(g * per * LANES, per * LANES)
            for d in order:
                copy = remote(
                    act.at[me, 1, :, cols],
                    act.at[me, 1, :, cols],
                    gs.at[d, 1 + g],
                    gr.at[d, 1 + g],
                    "fs",
                    flipped(me, d),
                )
                copy.start()
                shares.append(copy)

    other = lax.rem(core + 1, ntp)
    mine_at = pl.multiple_of(core * half_rows, half_rows)
    other_at = pl.multiple_of(other * half_rows, half_rows)

    def product(seq):
        return dot_rows(act[seq, 1], wa_ref[...]) + dot_rows(act[seq, 0], wp_ref[...])

    returns = []
    swaps = []
    turns = [0] + order
    for d in turns:
        seq = flipped(me, d)
        if d:
            with jax.named_scope("actwait"):
                for copy, at in zip(shares, order * (1 + groups)):
                    if at == d:
                        copy.wait_recv()
        with jax.named_scope("prod"):
            sums_ref[...] = product(seq)
            tsend[d] = sums_ref[pl.ds(other_at, half_rows)].astype(bf16)
        swap = remote(tsend.at[d], trecv.at[d], ts.at[d], tr.at[d], "tp", other)
        swap.start()
        swaps.append(swap)
        kept = sums_ref[pl.ds(mine_at, half_rows)]
        with jax.named_scope("swapwait"):
            swap.wait_recv()
        whole = (kept + trecv[d].astype(f32)).astype(bf16)
        if d:
            osend[d] = whole
            copy = remote(osend.at[d], orecv.at[me], os.at[d], orr.at[d], "fs", seq)
            copy.start()
            returns.append(copy)
        else:
            orecv[me] = whole
    with jax.named_scope("retwait"):
        for copy in returns:
            copy.wait_recv()
    for j in range(nfs):
        out_ref[0, :, j * channels : (j + 1) * channels] = orecv[j]
    for copy in shares + swaps + returns:
        copy.wait_send()
    for d in range(2):

        @pl.when(sends[d])
        def _():
            for g in range(groups):
                state_copy(d, g).wait_send()
            halo_copies[d].wait_send()
    finish_front()


def shards(
    inputs,
    input_norm_gain,
    receptance_matrix,
    key_matrix,
    value_matrix,
    pooling_input_weight,
    decay_lower_matrix,
    decay_raise_matrix,
    decay_offset_bias,
    removal_lower_matrix,
    removal_raise_matrix,
    removal_rate_bias,
    tempo_scale,
    sudden_decay_extra,
    head_norm_gain,
    group_mixing_weight,
    attention_output_matrix,
    pooling_output_matrix,
):
    nsp, nfs, ntp = lax.axis_size("sp"), lax.axis_size("fs"), lax.axis_size("tp")
    _, tokens, features = inputs.shape
    depth, channels = key_matrix.shape
    pairs = channels // LANES
    groups = pairs // PER
    wide = PER * LANES
    dma = pltpu.SemaphoreType.DMA
    rank = decay_lower_matrix.shape[1]
    rank2 = decay_raise_matrix.shape[0] * decay_raise_matrix.shape[1]
    anywhere = pl.BlockSpec(memory_space=pl.ANY)
    half = (nfs, tokens // ntp, depth)
    return pl.pallas_call(
        functools.partial(layer_kernel, nsp, nfs, ntp),
        out_shape=jax.ShapeDtypeStruct((1, tokens // ntp, features), bf16),
        in_specs=[VMEM] * 2
        + [anywhere] * 6
        + [VMEM] * 6
        + [anywhere, VMEM, anywhere, anywhere],
        out_specs=VMEM,
        scratch_shapes=[pltpu.VMEM((depth, channels), bf16)] * 4
        + [
            pltpu.VMEM((features, rank), bf16),
            pltpu.VMEM((features, rank), bf16),
            pltpu.VMEM(group_mixing_weight.shape, bf16),
            pltpu.VMEM(attention_output_matrix.shape, bf16),
            pltpu.VMEM(pooling_output_matrix.shape, bf16),
            dma((9,)),
            pltpu.VMEM((nfs, tokens, depth), bf16),
            pltpu.VMEM((nfs, tokens, depth), bf16),
            pltpu.VMEM((groups, 2, 3, tokens, wide), bf16),
            pltpu.VMEM((2, tokens, channels), bf16),
            pltpu.VMEM((groups, 3, tokens, wide), bf16),
            pltpu.VMEM((tokens, channels), bf16),
            pltpu.VMEM((groups, 2, 3, tokens, wide), bf16),
            pltpu.VMEM((2, tokens, channels), bf16),
            pltpu.VMEM((groups, 3, tokens, wide), bf16),
            pltpu.VMEM((tokens, channels), bf16),
            dma((nfs, ntp)),
            dma((nfs, ntp)),
            dma((groups + 1, 2)),
            dma((groups + 1, 2)),
            dma((groups + 1,)),
            dma((groups + 1,)),
            pltpu.VMEM((2, tokens, rank), bf16),
            pltpu.VMEM((tokens, channels), bf16),
            pltpu.VMEM((2, tokens, channels), bf16),
            pltpu.VMEM((tokens, channels), f32),
            pltpu.VMEM((2, pairs, LANES, LANES), bf16),
            pltpu.VMEM((2, pairs, HEAD, LANES), f32),
            pltpu.VMEM((2, HALO, channels), bf16),
            pltpu.VMEM((2, HALO, channels), bf16),
            pltpu.VMEM((2, groups, PER, HEAD, LANES), bf16),
            pltpu.VMEM((2, groups, PER, HEAD, LANES), bf16),
            pltpu.VMEM((nfs, 2, tokens, channels), bf16),
            pltpu.VMEM(half, bf16),
            pltpu.VMEM(half, bf16),
            pltpu.VMEM((tokens, depth), f32),
            pltpu.VMEM(half, bf16),
            pltpu.VMEM(half, bf16),
            dma((2,)),
            dma((2,)),
            dma((2, groups)),
            dma((2, groups)),
            dma((nfs, 1 + groups)),
            dma((nfs, 1 + groups)),
            dma((nfs,)),
            dma((nfs,)),
            dma((nfs,)),
            dma((nfs,)),
        ],
        compiler_params=pltpu.CompilerParams(
            collective_id=0, has_side_effects=True, vmem_limit_bytes=60 * 1024 * 1024
        ),
        name="layer",
    )(
        inputs,
        input_norm_gain,
        key_matrix,
        receptance_matrix,
        value_matrix,
        pooling_input_weight,
        decay_lower_matrix,
        removal_lower_matrix,
        decay_raise_matrix.reshape(rank2, channels),
        decay_offset_bias,
        removal_raise_matrix.reshape(rank2, channels),
        removal_rate_bias,
        tempo_scale[0],
        sudden_decay_extra[0],
        group_mixing_weight,
        head_norm_gain,
        attention_output_matrix,
        pooling_output_matrix,
    )


def solution(mesh):
    in_specs = (
        P("fs", "sp", None),
        P(),
        P("fs", "tp"),
        P("fs", "tp"),
        P("fs", "tp"),
        P("fs", "tp"),
        P(),
        P(None, None, "tp"),
        P(None, "tp"),
        P(),
        P(None, None, "tp"),
        P(None, "tp"),
        P("fs", None, "tp", "sp"),
        P("fs", None, "tp", "sp"),
        P("tp"),
        P("tp", None, None),
        P("fs", "tp"),
        P("fs", "tp"),
    )
    out_specs = P("fs", ("sp", "tp"), None)
    return jax.shard_map(shards, mesh=mesh, in_specs=in_specs, out_specs=out_specs, check_vma=False)
```

```python
import functools

import jax
import jax.numpy as jnp
from jax import lax
from jax.experimental import pallas as pl
from jax.experimental.pallas import tpu as pltpu
from jax.sharding import PartitionSpec as P

HEAD = 64
GROUP_WIDTH = 256
LANES = 128
BLOCK = 16
HALO = 16

norm_eps = 1e-06
head_eps = 0.00064
unit_eps = 1e-06
f32 = jnp.float32
bf16 = jnp.bfloat16
VMEM = pl.BlockSpec(memory_space=pltpu.VMEM)


def dot(left, right):
    return jnp.dot(left.astype(bf16), right.astype(bf16), preferred_element_type=f32)


def dot_general(left, right, dims):
    return lax.dot_general(
        left.astype(bf16), right.astype(bf16), (dims, ((), ())), preferred_element_type=f32
    )


def dot_rows(left, right):
    return dot_general(left, right, ((1,), (1,)))


def dot_cols(left, right):
    return dot_general(left, right, ((0,), (0,)))


def split_exact(cells, pieces):
    parts = []
    for _ in range(pieces - 1):
        high = cells.astype(bf16).astype(f32)
        parts.append(high)
        cells = cells - high
    return parts + [cells]


def remote(src, dst, send, recv, axis, peer):
    return pltpu.make_async_remote_copy(
        src_ref=src,
        dst_ref=dst,
        send_sem=send,
        recv_sem=recv,
        device_id={axis: peer},
        device_id_type=pl.DeviceIdType.MESH,
    )


def greet(barrier, axis, peer):
    pl.semaphore_signal(
        barrier, inc=1, device_id={axis: peer}, device_id_type=pl.DeviceIdType.MESH
    )


def flipped(at, bits):
    moved = at
    bit = 1
    while bit <= bits:
        if bits & bit:
            moved = moved + bit - 2 * bit * lax.rem(at // bit, 2)
        bit *= 2
    return moved


def front_part(
    n,
    x_ref,
    gain_ref,
    weights,
    lowers,
    loads,
    pool_ref,
    lat_ref,
    mine,
    cells,
    part,
    pool_part,
    onward,
    pool_onward,
    landed,
    pool_landed,
    joined,
    pool_joined,
    xs,
    xr,
    ps,
    pr,
    qs,
    qr,
    count,
    greet_line,
    meet_line,
    prepare,
    mix_group,
):
    me = lax.axis_index("fs")
    core, ntp = lax.axis_index("tp"), lax.axis_size("tp")
    width = x_ref.shape[2] // n
    plan = group_plan(part.shape[1])
    groups = len(plan)
    with jax.named_scope("xload"):
        for load in loads[:2]:
            load.wait()
    x = x_ref[0].astype(f32)
    with jax.named_scope("norm"):
        normed = (
            x
            * lax.rsqrt(jnp.mean(x * x, axis=-1, keepdims=True) + norm_eps)
            * gain_ref[...].astype(f32).reshape(1, -1)
        ).astype(bf16)
        for j in range(n):
            mine[j] = normed[:, j * width : (j + 1) * width]
    order = list(range(n - 1, 0, -1))
    lead = core == ntp - 1

    def row_copy(d):
        peer = flipped(me, d)
        return remote(mine.at[peer], cells.at[me], xs.at[d, 0], xr.at[d, 0], "fs", peer)

    def pass_copy(d, e):
        at = cells.at[flipped(me, d)]
        return remote(at, at, xs.at[d, 1 + e], xr.at[d, 1], "tp", e)

    with jax.named_scope("barrier"):

        @pl.when(lead)
        def _():
            pl.semaphore_wait(pltpu.get_barrier_semaphore(), count)
            for d in order:
                row_copy(d).start()

    with jax.named_scope("latent"):
        for load in loads[2:4]:
            load.wait()
        dl_ref, rl_ref = lowers
        decay = jnp.zeros((x.shape[0], dl_ref.shape[1]), f32)
        rate = jnp.zeros((x.shape[0], rl_ref.shape[1]), f32)
        for j in range(n):
            block = mine[j]
            decay = decay + dot(block, dl_ref[j * width : (j + 1) * width])
            rate = rate + dot(block, rl_ref[j * width : (j + 1) * width])
        lat_ref[0] = jnp.tanh(decay.astype(bf16).astype(f32)).astype(bf16)
        lat_ref[1] = rate.astype(bf16)
        for load in loads[4:]:
            load.wait()
    with jax.named_scope("xwait"):
        @pl.when(lead)
        def _():
            for d in order:
                row_copy(d).wait_recv()
                for e in range(ntp - 1):
                    pass_copy(d, e).start()

        @pl.when(jnp.logical_not(lead))
        def _():
            for d in order:
                pass_copy(d, 0).wait_recv()

        greet_line()

    first, second, across = routes(me, n, core)
    targets = (first, across)

    def span_of(g):
        at, count = plan[g]
        return pl.ds(at, count)

    def first_copy(g, slot):
        return remote(
            part.at[slot, span_of(g)],
            landed.at[slot, span_of(g)],
            ps.at[g, slot],
            pr.at[g, slot],
            "fs",
            first,
        )

    def first_pool(slot):
        return remote(
            pool_part.at[slot],
            pool_landed.at[slot],
            ps.at[groups, slot],
            pr.at[groups, slot],
            "fs",
            first,
        )

    def second_copy(g):
        return remote(
            onward.at[span_of(g)], joined.at[span_of(g)], qs.at[g], qr.at[g], "fs", second
        )

    second_pool = remote(
        pool_onward, pool_joined, qs.at[groups], qr.at[groups], "fs", second
    )

    def piece(m, g):
        at, count = plan[g]
        return weights[m][:, at * LANES : (at + count) * LANES]

    def beside(ref, g, m):
        at, count = plan[g]
        return jnp.concatenate([ref[p, m] for p in range(at, at + count)], 1).astype(f32)

    def keep(ref, g, m, cells):
        at, count = plan[g]
        for j in range(count):
            ref[at + j, m] = cells[:, j * LANES : (j + 1) * LANES].astype(bf16)

    with jax.named_scope("partials"):
        for g in range(groups):
            for slot in (1, 0):
                for m in range(3):
                    keep(part.at[slot], g, m, dot(cells[targets[slot]], piece(m, g)))
                first_copy(g, slot).start()

    def forward(g):
        with jax.named_scope(f"fwd{g}"):
            first_copy(g, 1).wait_recv()
            for m in range(3):
                keep(
                    onward, g, m, dot(cells[second], piece(m, g)) + beside(landed.at[1], g, m)
                )
            second_copy(g).start()

    def begin_pool():
        with jax.named_scope("beginpool"):
            for slot in (1, 0):
                pool_part[slot] = dot(cells[targets[slot]], weights[3][...]).astype(bf16)
                first_pool(slot).start()

    def forward_pool():
        with jax.named_scope("fwdpool"):
            first_pool(1).wait_recv()
            pool_onward[...] = (
                dot(cells[second], weights[3][...]) + pool_landed[1].astype(f32)
            ).astype(bf16)
            second_pool.start()

    def prep(g):
        with jax.named_scope(f"prep{g}"):
            prepare(g)

    def settle(g):
        with jax.named_scope(f"settle{g}"):
            first_copy(g, 0).wait_recv()
            second_copy(g).wait_recv()
        with jax.named_scope(f"mix{g}"):
            owned = [
                (
                    dot(mine[me], piece(m, g))
                    + beside(landed.at[0], g, m)
                    + beside(joined, g, m)
                ).astype(bf16)
                for m in range(3)
            ]
            mix_group(g, *owned)

    prep(0)
    forward(0)
    prep(1)
    forward(1)
    prep(2)
    meet_line()
    settle(0)
    forward(2)
    begin_pool()
    settle(1)
    forward_pool()
    settle(2)
    def settle_pool():
        with jax.named_scope("poolin"):
            first_pool(0).wait_recv()
            second_pool.wait_recv()
            pool_ref[...] = (
                dot(mine[me], weights[3][...])
                + pool_landed[0].astype(f32)
                + pool_joined[...].astype(f32)
            ).astype(bf16)

    def finish():
        @pl.when(lead)
        def _():
            for d in order:
                row_copy(d).wait_send()
                for e in range(ntp - 1):
                    pass_copy(d, e).wait_send()

        for g in range(groups):
            for slot in (1, 0):
                first_copy(g, slot).wait_send()
            second_copy(g).wait_send()
        for slot in (1, 0):
            first_pool(slot).wait_send()
        second_pool.wait_send()

    return settle_pool, finish


def group_plan(pairs):
    quarter = pairs // 4
    return [(0, quarter), (quarter, pairs - 2 * quarter), (pairs - quarter, quarter)]


def routes(me, n, core):
    low, high = flipped(me, 1), flipped(me, n // 2)
    odd = lax.rem(core, 2)
    return low + odd * (high - low), high + odd * (low - high), flipped(me, n // 2 + 1)


def cut(cells, j):
    return cells[:, j * LANES : (j + 1) * LANES]


def live_rows(d, i, tokens):
    return slice(0, (i + 1) * BLOCK) if d == 0 else slice(i * BLOCK, tokens)


def prepare_group(
    start,
    per,
    lat_ref,
    draise_ref,
    dbias_ref,
    rraise_ref,
    rbias_ref,
    tempo_ref,
    extra_ref,
    fade_ref,
    grow_ref,
):
    tokens = lat_ref.shape[1]
    wide = per * LANES
    lanes = slice(start * LANES, start * LANES + wide)
    lane = lax.broadcasted_iota(jnp.int32, (tokens, LANES), 1)
    row = lax.broadcasted_iota(jnp.int32, (tokens, LANES), 0)
    head0 = lane < HEAD
    heads = tempo_ref.shape[1]
    spread = (
        lax.broadcasted_iota(jnp.int32, (heads, wide), 0)
        == 2 * start + lax.broadcasted_iota(jnp.int32, (heads, wide), 1) // HEAD
    ).astype(f32)
    spread = jnp.concatenate([spread] * 3, 0)

    def spread_out(cells):
        return dot_cols(jnp.concatenate(split_exact(cells, 3), 0), spread)

    blocks = tokens // BLOCK
    zero_row = jnp.zeros((1, wide), f32)
    for d in range(2):
        lat_mask = head0 if d == 0 else ~head0
        lat_d = jnp.where(lat_mask, lat_ref[0].astype(f32), 0.0)
        lat_r = jnp.where(lat_mask, lat_ref[1].astype(f32), 0.0)
        pre = dbias_ref[d : d + 1, lanes] + dot(lat_d, draise_ref[:, lanes])
        velocity = jax.nn.sigmoid(pre) * 0.6065306597126334
        ld = -velocity * spread_out(tempo_ref[d]) + spread_out(extra_ref[d])
        rate = jax.nn.sigmoid(rbias_ref[d : d + 1, lanes] + dot(lat_r, rraise_ref[:, lanes]))
        upto = (lane <= row) if d == 0 else (lane >= row)
        tri = upto.astype(f32).astype(bf16)
        inner = dot(jnp.concatenate([tri, tri], 1), jnp.concatenate(split_exact(ld, 2), 0))
        excl = inner - ld
        last = inner[tokens - 1 : tokens] if d == 0 else inner[0:1]
        fade_ref[d, 0, :, lanes] = jnp.exp(excl)
        fade_ref[d, 1, :, lanes] = jnp.exp(inner)
        fade_ref[d, 2, :, lanes] = jnp.exp(last - inner) * rate
        for i in range(blocks):
            lo, hi = i * BLOCK, (i + 1) * BLOCK
            if d == 0:
                base = inner[lo - 1 : lo] if i > 0 else zero_row
            else:
                base = inner[hi : hi + 1] if i < blocks - 1 else zero_row
            live = live_rows(d, i, tokens)
            fade_ref[d, 3, lo:hi, lanes] = jnp.exp(excl[lo:hi] - base)
            fade_ref[d, 4, lo:hi, lanes] = jnp.exp(inner[lo:hi] - base)
            grow = jnp.exp(jnp.minimum(base - inner[live], 80.0))
            grow_ref[d, i, live, lanes] = grow * rate[live]


def mix_group(
    start,
    key,
    receptance,
    value,
    fade_ref,
    grow_ref,
    query_ref,
    local_ref,
    transfer_ref,
    carried_ref,
):
    tokens, wide = key.shape
    per = wide // LANES
    kf = key.astype(f32)
    rf = receptance.astype(f32)
    lane = lax.broadcasted_iota(jnp.int32, (tokens, LANES), 1)
    row = lax.broadcasted_iota(jnp.int32, (tokens, LANES), 0)
    head0 = lane < HEAD
    only = [head0.astype(f32).astype(bf16), (~head0).astype(f32).astype(bf16)]
    blank = jnp.zeros((tokens, LANES), bf16)

    def both_heads(cells):
        return jnp.concatenate([cells * only[0], cells * only[1]], 0)

    def rows_for_heads(cells):
        return jnp.concatenate(
            [jnp.concatenate([cut(cells, i) * o for i in range(cells.shape[1] // LANES)], 1) for o in only], 0
        )

    units = []
    for j in range(per):
        kj = cut(kf, j)
        k2 = kj * kj
        s0 = jnp.sum(jnp.where(head0, k2, 0.0), axis=-1, keepdims=True)
        s1 = jnp.sum(jnp.where(head0, 0.0, k2), axis=-1, keepdims=True)
        units.append(kj * lax.rsqrt(jnp.where(head0, s0, s1) + unit_eps))
    blocks = tokens // BLOCK
    eye = (row == lane).astype(f32)
    sizes = []
    size = 1
    while size < tokens:
        sizes.append(size)
        size *= 2

    def level_mask(k):
        return ((row >> (k + 1)) == (lane >> (k + 1))) & ((row >> k) != (lane >> k))

    ways = [[] for _ in range(per)]
    for d in range(2):
        upto = (lane <= row) if d == 0 else (lane >= row)
        strict = (lane < row) if d == 0 else (lane > row)
        for j in range(per):
            at = slice((start + j) * LANES, (start + j + 1) * LANES)
            unit, kj, rj = units[j], cut(kf, j), cut(rf, j)
            aheads = unit * fade_ref[d, 3, :, at]
            queries = rj * fade_ref[d, 4, :, at]
            firsts = [
                jnp.where(head0, aheads, 0.0).astype(bf16),
                jnp.where(head0, 0.0, aheads).astype(bf16),
                jnp.where(head0, queries, 0.0).astype(bf16),
                jnp.where(head0, 0.0, queries).astype(bf16),
            ]
            grams = []
            for i in range(blocks):
                lo, hi = i * BLOCK, (i + 1) * BLOCK
                live = live_rows(d, i, tokens)
                grow = grow_ref[d, i, live, at]
                rest = tokens - grow.shape[0]

                def filled(cells):
                    cells = cells.astype(bf16)
                    if not rest:
                        return cells
                    empty = jnp.zeros((rest, LANES), bf16)
                    return jnp.concatenate([cells, empty] if d == 0 else [empty, cells], 0)

                right = jnp.concatenate(
                    [filled(unit[live] * grow), filled(kj[live] * grow)], 0
                )
                grams.append(dot_rows(jnp.concatenate([f[lo:hi] for f in firsts], 0), right))

            def gathered(place, at, mask):
                rows = jnp.concatenate(
                    [
                        gram[place * BLOCK : (place + 1) * BLOCK, at * tokens : (at + 1) * tokens]
                        for gram in grams
                    ],
                    0,
                )
                return jnp.where(mask, rows, 0.0)

            way = dict()
            way["link"] = [gathered(h, 0, strict) for h in range(2)]
            way["write"] = [gathered(h, 1, strict).astype(bf16) for h in range(2)]
            way["read"] = [gathered(2 + h, 0, upto).astype(bf16) for h in range(2)]
            way["read_write"] = [gathered(2 + h, 1, upto).astype(bf16) for h in range(2)]
            ways[j].append(way)

    links = [link for j in range(per) for way in ways[j] for link in way["link"]]
    mask = level_mask(0)
    inverses = [(eye - jnp.where(mask, a, 0.0)).astype(bf16) for a in links]
    links = [a.astype(bf16) for a in links]

    def products(lefts, rights):
        out = []
        for i in range(0, len(lefts), 2):
            result = dot(
                jnp.concatenate(lefts[i : i + 2], 1),
                jnp.concatenate(
                    [
                        jnp.concatenate([rights[i], blank], 1),
                        jnp.concatenate([blank, rights[i + 1]], 1),
                    ],
                    0,
                ),
            ).astype(bf16)
            out += [cut(result, 0), cut(result, 1)]
        return out

    def level_bits(k):
        return level_mask(k).astype(f32).astype(bf16)

    for k in range(1, len(sizes), 2):
        if k + 1 == len(sizes):
            mask = level_bits(k)
            firsts = products(inverses, [a * mask for a in links])
            steps = products(firsts, inverses)
            inverses = [t - u for t, u in zip(inverses, steps)]
            continue
        mask = level_bits(k) + level_bits(k + 1)
        firsts = products(inverses, [a * mask for a in links])
        steps = products(firsts, inverses)
        squares = products(firsts, firsts)
        inverses = [t - u for t, u in zip(inverses, steps)]
        inverses = [t + u for t, u in zip(inverses, products(squares, inverses))]

    block_diag = (row < HEAD) == head0
    for j in range(per):
        pair = start + j
        vj = cut(value, j)
        stacked = both_heads(vj)
        sums = dot(
            jnp.concatenate(
                [
                    jnp.concatenate(way[name], 1)
                    for way in ways[j]
                    for name in ("write", "read_write")
                ],
                0,
            ),
            stacked,
        )
        local = sums[tokens : 2 * tokens] + sums[3 * tokens :]
        at = slice(pair * LANES, (pair + 1) * LANES)
        for d, way in enumerate(ways[j]):
            ahead = units[j] * fade_ref[d, 0, :, at]
            query = cut(rf, j) * fade_ref[d, 1, :, at]
            edge_row = tokens - 1 if d == 0 else 0
            last = fade_ref[d, 1, edge_row : edge_row + 1, at]
            base = sums[2 * d * tokens : (2 * d + 1) * tokens]
            rhs = jnp.concatenate([ahead.astype(bf16), base.astype(bf16)], 1)
            place = 4 * j + 2 * d
            solved = -dot(jnp.concatenate(inverses[place : place + 2], 1), rows_for_heads(rhs))
            solved = solved.astype(bf16)
            tail = fade_ref[d, 2, :, at]
            remove_tail = (units[j] * tail).astype(bf16)
            write_tail = (cut(kf, j) * tail).astype(bf16)
            seen = dot(jnp.concatenate(way["read"], 1), rows_for_heads(solved))
            query_ref[d, :, pair * LANES : (pair + 1) * LANES] = (query + cut(seen, 0)).astype(bf16)
            local = local + cut(seen, 1)
            onto = dot_cols(remove_tail, solved)
            transfer = jnp.where(block_diag, cut(onto, 0), 0.0) + eye * last
            transfer_ref[d, pair] = transfer.astype(bf16)
            carried = cut(onto, 1) + dot_cols(write_tail, vj)
            carried_ref[d, pair] = jnp.where(
                head0[:HEAD], carried[:HEAD], carried[HEAD:]
            )
        local_ref[:, pair * LANES : (pair + 1) * LANES] = local


def layer_kernel(
    nsp,
    nfs,
    ntp,
    x_hbm,
    in_gain_hbm,
    wk_hbm,
    wr_hbm,
    wv_hbm,
    wi_hbm,
    dl_hbm,
    rl_hbm,
    draise_hbm,
    dbias_hbm,
    rraise_hbm,
    rbias_hbm,
    tempo_hbm,
    extra_hbm,
    mix_hbm,
    gain_hbm,
    wa_hbm,
    wp_hbm,
    out_hbm,
    x_ref,
    in_gain_ref,
    draise_ref,
    dbias_ref,
    rraise_ref,
    rbias_ref,
    tempo_ref,
    extra_ref,
    gain_ref,
    wk_ref,
    wr_ref,
    wv_ref,
    wi_ref,
    dl_ref,
    rl_ref,
    mix_ref,
    wa_ref,
    wp_ref,
    loaded,
    mine,
    cells,
    part,
    pool_part,
    onward,
    pool_onward,
    landed,
    pool_landed,
    joined,
    pool_joined,
    xs,
    xr,
    ready,
    ps,
    pr,
    qs,
    qr,
    lat_ref,
    fade_ref,
    grow_ref,
    pool_ref,
    query_ref,
    local_ref,
    transfer_ref,
    carried_ref,
    edge,
    halo,
    incoming,
    leaving,
    near_state,
    near_map,
    skipped,
    onto_next,
    act,
    tsend,
    trecv,
    sums_ref,
    osend,
    hs,
    hr,
    ss,
    sr,
    gs,
    gr,
    ts,
    tr,
    os,
    orr,
):
    z = lax.axis_index("sp")
    me = lax.axis_index("fs")
    core = lax.axis_index("tp")
    tokens, channels = local_ref.shape
    depth = wa_ref.shape[0]
    half_rows = tokens // ntp
    has_prev = z > 0
    has_next = z < nsp - 1
    prev = jnp.maximum(z - 1, 0)
    after = jnp.minimum(z + 1, nsp - 1)
    prev2 = jnp.maximum(z - 2, 0)
    after2 = jnp.minimum(z + 2, nsp - 1)

    barrier = pltpu.get_barrier_semaphore()
    lead = core == ntp - 1

    @pl.when(lead)
    def _():
        for d in range(1, nfs):
            greet(barrier, "fs", flipped(me, d))

    @pl.when(jnp.logical_not(lead))
    def _():
        greet(barrier, "tp", ntp - 1)

    near = ((has_prev, prev), (has_next, after), (z > 1, prev2), (z < nsp - 2, after2))

    def greet_line():
        @pl.when(core == 0)
        def _():
            for there, peer in near:
                pl.when(there)(lambda: greet(barrier, "sp", peer))

    def meet_line():
        @pl.when(core == 0)
        def _():
            count = 0
            for there, _ in near:
                count = count + jnp.where(there, 1, 0)
            pl.semaphore_wait(barrier, count)
            for e in range(1, ntp):
                greet(ready, "tp", e)

        @pl.when(core != 0)
        def _():
            pl.semaphore_wait(ready, 1)

    small = (draise_hbm, dbias_hbm, rraise_hbm, rbias_hbm, tempo_hbm, extra_hbm, gain_hbm)
    sources = (x_hbm, in_gain_hbm, dl_hbm, rl_hbm, wk_hbm, wr_hbm, wv_hbm, wi_hbm)
    sources += small + (mix_hbm, wa_hbm, wp_hbm)
    small = (draise_ref, dbias_ref, rraise_ref, rbias_ref, tempo_ref, extra_ref, gain_ref)
    targets = (x_ref, in_gain_ref, dl_ref, rl_ref, wk_ref, wr_ref, wv_ref, wi_ref)
    targets += small + (mix_ref, wa_ref, wp_ref)
    loads = [
        pltpu.make_async_copy(source, target, loaded.at[i])
        for i, (source, target) in enumerate(zip(sources, targets))
    ]
    for load in loads:
        load.start()
    plan = group_plan(transfer_ref.shape[1])
    groups = len(plan)

    STATE, NEAR, MAP, SKIP = range(4)
    places = (z, nsp - 1 - z)
    odd = [lax.rem(place, 2) == 1 for place in places]

    def both(*tests):
        result = tests[0]
        for test in tests[1:]:
            result = jnp.logical_and(result, test)
        return result

    def state_copy(kind, d, g):
        span = pl.ds(plan[g][0], plan[g][1])
        source = (onto_next, leaving, transfer_ref, onto_next)[kind]
        target = (incoming, near_state, near_map, skipped)[kind]
        step = (after, prev) if kind != SKIP else (after2, prev2)
        return remote(
            source.at[d, span],
            target.at[d, span],
            ss.at[kind, d, g],
            sr.at[kind, d, g],
            "sp",
            step[d],
        )

    def starts(d):
        place = places[d]
        goes = place < nsp - 1
        return (
            (STATE, both(odd[d], goes)),
            (NEAR, both(jnp.logical_not(odd[d]), goes)),
            (MAP, both(jnp.logical_not(odd[d]), goes, place > 0)),
            (SKIP, both(odd[d], place < nsp - 2)),
        )

    halo_copies = [
        remote(edge.at[1], halo.at[0], hs.at[0], hr.at[0], "sp", after),
        remote(edge.at[0], halo.at[1], hs.at[1], hr.at[1], "sp", prev),
    ]
    sends = [has_next, has_prev]
    takes = [has_prev, has_next]

    def pairs_of(g):
        return range(plan[g][0], plan[g][0] + plan[g][1])

    def mix_step(g, *operands):
        mix_group(plan[g][0], *operands)
        for d in range(2):

            @pl.when(places[d] == 0)
            def _():
                for p in pairs_of(g):
                    incoming[d, p] = jnp.zeros_like(incoming[d, p])

            for p in pairs_of(g):
                leaving[d, p] = carried_ref[d, p].astype(bf16)
            for kind, goes in starts(d)[NEAR : MAP + 1]:
                pl.when(goes)(lambda: state_copy(kind, d, g).start())

    def doubled(state):
        top0 = lax.broadcasted_iota(jnp.int32, state.shape, 1) < HEAD
        state = state.astype(f32)
        return jnp.concatenate([jnp.where(top0, state, 0.0), jnp.where(top0, 0.0, state)], 0)

    def moved(by, state):
        both_halves = dot(by, doubled(state))
        return both_halves[:HEAD] + both_halves[HEAD:]

    def relay(d, g):
        place = places[d]

        @pl.when(odd[d])
        def _():
            state_copy(NEAR, d, g).wait_recv()

            @pl.when(place == 1)
            def _():
                for p in pairs_of(g):
                    incoming[d, p] = near_state[d, p]

            @pl.when(place > 1)
            def _():
                state_copy(MAP, d, g).wait_recv()
                state_copy(SKIP, d, g).wait_recv()
                for p in pairs_of(g):
                    incoming[d, p] = (
                        moved(near_map[d, p], skipped[d, p]) + near_state[d, p].astype(f32)
                    ).astype(bf16)

            @pl.when(place < nsp - 1)
            def _():
                for p in pairs_of(g):
                    onto_next[d, p] = (
                        moved(transfer_ref[d, p], incoming[d, p]) + carried_ref[d, p]
                    ).astype(bf16)
                state_copy(STATE, d, g).start()
                pl.when(place < nsp - 2)(lambda: state_copy(SKIP, d, g).start())

        @pl.when(both(jnp.logical_not(odd[d]), place > 0))
        def _():
            state_copy(STATE, d, g).wait_recv()

    early = 2 * z < nsp

    def relays(near, g):
        @pl.when(early)
        def _():
            relay(0 if near else 1, g)

        @pl.when(jnp.logical_not(early))
        def _():
            relay(1 if near else 0, g)

    settle_pool, finish_front = front_part(
        nfs,
        x_ref,
        in_gain_ref,
        (wk_ref, wr_ref, wv_ref, wi_ref),
        (dl_ref, rl_ref),
        loads[:15],
        pool_ref,
        lat_ref,
        mine,
        cells,
        part,
        pool_part,
        onward,
        pool_onward,
        landed,
        pool_landed,
        joined,
        pool_joined,
        xs,
        xr,
        ps,
        pr,
        qs,
        qr,
        nfs + ntp - 2,
        greet_line,
        meet_line,
        lambda g: prepare_group(
            plan[g][0],
            plan[g][1],
            lat_ref,
            draise_ref,
            dbias_ref,
            rraise_ref,
            rbias_ref,
            tempo_ref,
            extra_ref,
            fade_ref,
            grow_ref,
        ),
        lambda g, key, receptance, value: mix_step(
            g,
            key,
            receptance,
            value,
            fade_ref,
            grow_ref,
            query_ref,
            local_ref,
            transfer_ref,
            carried_ref,
        ),
    )
    for load in loads[15:]:
        load.wait()
    first, second, across = routes(me, nfs, core)

    def act_part(seq, k):
        if k == 0:
            return act.at[seq, 0]
        at, count = plan[k - 1]
        return act.at[seq, 1, :, pl.ds(at * LANES, count * LANES)]

    def share(k, seq, way, peer):
        return remote(
            act_part(seq, k), act_part(seq, k), gs.at[k, way], gr.at[k, way], "fs", peer
        )

    whole_way = groups

    def share_out(k):
        if k == whole_way:
            share(k, me, 2, across).start()
        share(k, me, 0, first).start()
        share(k, me, 1, second).start()

    def pass_on(k):
        share(k, first, 0, first).wait_recv()
        if k != whole_way:
            share(k, first, 2, second).start()

    head0 = lax.broadcasted_iota(jnp.int32, (tokens, LANES), 1) < HEAD

    def head_mean(values):
        low = jnp.sum(jnp.where(head0, values, 0.0), axis=-1, keepdims=True)
        high = jnp.sum(jnp.where(head0, 0.0, values), axis=-1, keepdims=True)
        return jnp.where(head0, low, high) * (1.0 / HEAD)

    def finish_group(g):
        with jax.named_scope(f"relayB{g}"):
            relays(False, g)
        with jax.named_scope(f"readout{g}"):
            for p in pairs_of(g):
                lanes = slice(p * LANES, (p + 1) * LANES)
                readout = local_ref[:, lanes]
                for d in range(2):
                    readout = readout + dot(query_ref[d, :, lanes], doubled(incoming[d, p]))
                centred = readout - head_mean(readout)
                scaled = centred * lax.rsqrt(head_mean(centred * centred) + head_eps)
                act[me, 1, :, lanes] = (
                    scaled * gain_ref[lanes].astype(f32).reshape(1, -1)
                ).astype(bf16)
            share_out(1 + g)

    for g in range(groups - 1):
        with jax.named_scope(f"relayA{g}"):
            relays(True, g)
    settle_pool()
    edge[0] = pool_ref[:HALO]
    edge[1] = pool_ref[tokens - HALO :]
    for d in range(2):
        pl.when(sends[d])(lambda: halo_copies[d].start())
    with jax.named_scope("relayAlast"):
        relays(True, groups - 1)
    for g in range(groups - 1):
        finish_group(g)
    with jax.named_scope("halo"):
        for d in range(2):

            @pl.when(takes[d])
            def _():
                halo_copies[d].wait_recv()

            @pl.when(jnp.logical_not(takes[d]))
            def _():
                halo[d] = jnp.zeros_like(halo[d])

    span = tokens + 2 * HALO
    rim = jnp.concatenate([halo[0], pool_ref[...], halo[1]], 0)
    here = lax.broadcasted_iota(jnp.int32, (tokens, span), 0)
    there = lax.broadcasted_iota(jnp.int32, (tokens, span), 1) - HALO
    position = z * tokens + lax.broadcasted_iota(jnp.int32, (tokens, GROUP_WIDTH), 0)
    length = tokens * nsp
    groups_here = channels // GROUP_WIDTH
    for member in range(groups_here):
        cols = slice(member * GROUP_WIDTH, (member + 1) * GROUP_WIDTH)
        reach = jnp.left_shift(1, core * groups_here + member)
        window = jnp.where((there >= here - reach) & (there < here + reach), 1.0, 0.0)
        total = dot(window, rim[:, cols])
        size = (
            jnp.minimum(position + reach, length) - jnp.maximum(position - reach, 0)
        ).astype(f32)
        diff = (total / size - pool_ref[:, cols].astype(f32)).astype(bf16)
        act[me, 0, :, cols] = dot(diff, mix_ref[member]).astype(bf16)
    share_out(0)

    finish_group(groups - 1)

    other = lax.rem(core + 1, ntp)
    mine_at = pl.multiple_of(core * half_rows, half_rows)
    other_at = pl.multiple_of(other * half_rows, half_rows)

    def product(seq, k):
        if k == 0:
            return dot_rows(act[seq, 0], wp_ref[...])
        at, count = plan[k - 1]
        cols = slice(at * LANES, (at + count) * LANES)
        return dot_rows(act[seq, 1, :, cols], wa_ref[:, cols])

    def swap_of(i):
        return remote(tsend.at[i], trecv.at[i], ts.at[i], tr.at[i], "tp", other)

    def offer(i, total):
        sums_ref[i] = total
        tsend[i] = sums_ref[i, pl.ds(other_at, half_rows)].astype(bf16)
        swap_of(i).start()

    place = out_hbm.at[0, :, pl.ds(pl.multiple_of(me * depth, depth), depth)]

    def back(i, seq):
        return remote(osend.at[i], place, os.at[i], orr.at[i], "fs", seq)

    own_out = pltpu.make_async_copy(osend.at[0], place, os.at[0])

    def settle_out(i, seq):
        swap_of(i).wait_recv()
        osend[i] = (
            sums_ref[i, pl.ds(mine_at, half_rows)] + trecv[i].astype(f32)
        ).astype(bf16)
        (back(i, seq) if i else own_out).start()

    with jax.named_scope("prodown"):
        offer(0, sum(product(me, k) for k in range(1 + groups)))
    peers = ((1, flipped(me, 1)), (2, flipped(me, nfs // 2)), (3, across))
    turn = list(range(1, groups)) + [0]
    for k in turn:
        with jax.named_scope(f"pass{k}"):
            pass_on(k)
            share(k, second, 1, second).wait_recv()
        with jax.named_scope(f"prod{k}"):
            for i, seq in peers[:2]:
                sums_ref[i] = product(seq, k) + (sums_ref[i] if k != turn[0] else 0.0)
        if k == turn[0]:
            settle_out(0, me)
    k = groups
    with jax.named_scope(f"wait{k}1"):
        share(k, first, 0, first).wait_recv()
        share(k, second, 1, second).wait_recv()
    for i, seq in peers[:2]:
        with jax.named_scope(f"prod{k}{i}"):
            offer(i, product(seq, k) + sums_ref[i])
    for k in turn + [groups]:
        with jax.named_scope(f"wait{k}3"):
            share(k, across, 2, across).wait_recv()
        with jax.named_scope(f"prod{k}3"):
            total = product(across, k) + (sums_ref[3] if k != turn[0] else 0.0)
            if k < groups:
                sums_ref[3] = total
            else:
                offer(3, total)
        if k == turn[0]:
            for i, seq in peers[:2]:
                with jax.named_scope(f"swapwait{i}"):
                    settle_out(i, seq)
    with jax.named_scope("swapwait3"):
        settle_out(3, across)
    with jax.named_scope("retwait"):
        for i, seq in peers:
            back(i, seq).wait_recv()
    own_out.wait()
    for k in range(1 + groups):
        for way in range(3):
            share(k, me, way, first).wait_send()
    for i in range(1 + len(peers)):
        swap_of(i).wait_send()
    for i, seq in peers:
        back(i, seq).wait_send()
    for d in range(2):

        @pl.when(sends[d])
        def _():
            halo_copies[d].wait_send()

        for kind, goes in starts(d):

            @pl.when(goes)
            def _():
                for g in range(groups):
                    state_copy(kind, d, g).wait_send()
    finish_front()


def shards(
    inputs,
    input_norm_gain,
    receptance_matrix,
    key_matrix,
    value_matrix,
    pooling_input_weight,
    decay_lower_matrix,
    decay_raise_matrix,
    decay_offset_bias,
    removal_lower_matrix,
    removal_raise_matrix,
    removal_rate_bias,
    tempo_scale,
    sudden_decay_extra,
    head_norm_gain,
    group_mixing_weight,
    attention_output_matrix,
    pooling_output_matrix,
):
    nsp, nfs, ntp = lax.axis_size("sp"), lax.axis_size("fs"), lax.axis_size("tp")
    _, tokens, features = inputs.shape
    depth, channels = key_matrix.shape
    pairs = channels // LANES
    groups = len(group_plan(pairs))
    dma = pltpu.SemaphoreType.DMA
    rank = decay_lower_matrix.shape[1]
    rank2 = decay_raise_matrix.shape[0] * decay_raise_matrix.shape[1]
    anywhere = pl.BlockSpec(memory_space=pl.ANY)
    half = (nfs, tokens // ntp, depth)
    return pl.pallas_call(
        functools.partial(layer_kernel, nsp, nfs, ntp),
        out_shape=pltpu.VMEM((1, tokens // ntp, features), bf16),
        in_specs=[anywhere] * 18,
        out_specs=anywhere,
        scratch_shapes=[
            pltpu.VMEM(inputs.shape, bf16),
            pltpu.VMEM(input_norm_gain.shape, bf16),
            pltpu.VMEM((rank2, channels), bf16),
            pltpu.VMEM(decay_offset_bias.shape, f32),
            pltpu.VMEM((rank2, channels), bf16),
            pltpu.VMEM(removal_rate_bias.shape, f32),
            pltpu.VMEM(tempo_scale.shape[1:], f32),
            pltpu.VMEM(sudden_decay_extra.shape[1:], f32),
            pltpu.VMEM(head_norm_gain.shape, bf16),
        ]
        + [pltpu.VMEM((depth, channels), bf16)] * 4
        + [
            pltpu.VMEM((features, rank), bf16),
            pltpu.VMEM((features, rank), bf16),
            pltpu.VMEM(group_mixing_weight.shape, bf16),
            pltpu.VMEM(attention_output_matrix.shape, bf16),
            pltpu.VMEM(pooling_output_matrix.shape, bf16),
            dma((18,)),
            pltpu.VMEM((nfs, tokens, depth), bf16),
            pltpu.VMEM((nfs, tokens, depth), bf16),
            pltpu.VMEM((2, pairs, 3, tokens, LANES), bf16),
            pltpu.VMEM((2, tokens, channels), bf16),
            pltpu.VMEM((pairs, 3, tokens, LANES), bf16),
            pltpu.VMEM((tokens, channels), bf16),
            pltpu.VMEM((2, pairs, 3, tokens, LANES), bf16),
            pltpu.VMEM((2, tokens, channels), bf16),
            pltpu.VMEM((pairs, 3, tokens, LANES), bf16),
            pltpu.VMEM((tokens, channels), bf16),
            dma((nfs, ntp)),
            dma((nfs, 2)),
            pltpu.SemaphoreType.REGULAR,
            dma((groups + 1, 2)),
            dma((groups + 1, 2)),
            dma((groups + 1,)),
            dma((groups + 1,)),
            pltpu.VMEM((2, tokens, rank), bf16),
            pltpu.VMEM((2, 5, tokens, channels), f32),
            pltpu.VMEM((2, tokens // BLOCK, tokens, channels), f32),
            pltpu.VMEM((tokens, channels), bf16),
            pltpu.VMEM((2, tokens, channels), bf16),
            pltpu.VMEM((tokens, channels), f32),
            pltpu.VMEM((2, pairs, LANES, LANES), bf16),
            pltpu.VMEM((2, pairs, HEAD, LANES), f32),
            pltpu.VMEM((2, HALO, channels), bf16),
            pltpu.VMEM((2, HALO, channels), bf16),
            pltpu.VMEM((2, pairs, HEAD, LANES), bf16),
            pltpu.VMEM((2, pairs, HEAD, LANES), bf16),
            pltpu.VMEM((2, pairs, HEAD, LANES), bf16),
            pltpu.VMEM((2, pairs, LANES, LANES), bf16),
            pltpu.VMEM((2, pairs, HEAD, LANES), bf16),
            pltpu.VMEM((2, pairs, HEAD, LANES), bf16),
            pltpu.VMEM((nfs, 2, tokens, channels), bf16),
            pltpu.VMEM(half, bf16),
            pltpu.VMEM(half, bf16),
            pltpu.VMEM((nfs, tokens, depth), f32),
            pltpu.VMEM(half, bf16),
            dma((2,)),
            dma((2,)),
            dma((4, 2, groups)),
            dma((4, 2, groups)),
            dma((1 + groups, 3)),
            dma((1 + groups, 3)),
            dma((nfs,)),
            dma((nfs,)),
            dma((nfs,)),
            dma((nfs,)),
        ],
        compiler_params=pltpu.CompilerParams(
            collective_id=0, has_side_effects=True, vmem_limit_bytes=60 * 1024 * 1024
        ),
        name="layer",
    )(
        inputs,
        input_norm_gain,
        key_matrix,
        receptance_matrix,
        value_matrix,
        pooling_input_weight,
        decay_lower_matrix,
        removal_lower_matrix,
        decay_raise_matrix.reshape(rank2, channels),
        decay_offset_bias,
        removal_raise_matrix.reshape(rank2, channels),
        removal_rate_bias,
        tempo_scale[0],
        sudden_decay_extra[0],
        group_mixing_weight,
        head_norm_gain,
        attention_output_matrix,
        pooling_output_matrix,
    )


def solution(mesh):
    in_specs = (
        P("fs", "sp", None),
        P(),
        P("fs", "tp"),
        P("fs", "tp"),
        P("fs", "tp"),
        P("fs", "tp"),
        P(),
        P(None, None, "tp"),
        P(None, "tp"),
        P(),
        P(None, None, "tp"),
        P(None, "tp"),
        P("fs", None, "tp", "sp"),
        P("fs", None, "tp", "sp"),
        P("tp"),
        P("tp", None, None),
        P("fs", "tp"),
        P("fs", "tp"),
    )
    out_specs = P("fs", ("sp", "tp"), None)
    return jax.shard_map(shards, mesh=mesh, in_specs=in_specs, out_specs=out_specs, check_vma=False)
```

```python
import functools

import jax
import jax.numpy as jnp
from jax import lax
from jax.experimental import pallas as pl
from jax.experimental.pallas import tpu as pltpu
from jax.sharding import PartitionSpec as P

HEAD = 64
GROUP_WIDTH = 256
LANES = 128
BLOCK = 16
HALO = 16

norm_eps = 1e-06
head_eps = 0.00064
unit_eps = 1e-06
f32 = jnp.float32
bf16 = jnp.bfloat16
VMEM = pl.BlockSpec(memory_space=pltpu.VMEM)


def dot(left, right):
    return jnp.dot(left.astype(bf16), right.astype(bf16), preferred_element_type=f32)


def dot_general(left, right, dims):
    return lax.dot_general(
        left.astype(bf16), right.astype(bf16), (dims, ((), ())), preferred_element_type=f32
    )


def dot_rows(left, right):
    return dot_general(left, right, ((1,), (1,)))


def dot_cols(left, right):
    return dot_general(left, right, ((0,), (0,)))


def split_exact(cells, pieces):
    parts = []
    for _ in range(pieces - 1):
        high = cells.astype(bf16).astype(f32)
        parts.append(high)
        cells = cells - high
    return parts + [cells]


def remote(src, dst, send, recv, axis, peer):
    return pltpu.make_async_remote_copy(
        src_ref=src,
        dst_ref=dst,
        send_sem=send,
        recv_sem=recv,
        device_id={axis: peer},
        device_id_type=pl.DeviceIdType.MESH,
    )


def greet(barrier, axis, peer):
    pl.semaphore_signal(
        barrier, inc=1, device_id={axis: peer}, device_id_type=pl.DeviceIdType.MESH
    )


def flipped(at, bits):
    moved = at
    bit = 1
    while bit <= bits:
        if bits & bit:
            moved = moved + bit - 2 * bit * lax.rem(at // bit, 2)
        bit *= 2
    return moved


def front_part(
    n,
    x_ref,
    gain_ref,
    weights,
    lowers,
    loads,
    pool_ref,
    lat_ref,
    mine,
    cells,
    part,
    pool_part,
    own_part,
    onward,
    pool_onward,
    landed,
    pool_landed,
    joined,
    pool_joined,
    xs,
    xr,
    loaded,
    pr,
    qr,
    count,
    greet_line,
    meet_line,
    send_rims,
    own_rims,
    prepare,
    mix_group,
):
    me = lax.axis_index("fs")
    core, ntp = lax.axis_index("tp"), lax.axis_size("tp")
    width = x_ref.shape[2] // n
    plan = group_plan(part.shape[1])
    groups = len(plan)
    with jax.named_scope("xload"):
        for load in loads[:2]:
            load.wait()
    x = x_ref[0].astype(f32)
    with jax.named_scope("norm"):
        normed = (
            x
            * lax.rsqrt(jnp.mean(x * x, axis=-1, keepdims=True) + norm_eps)
            * gain_ref[...].astype(f32).reshape(1, -1)
        ).astype(bf16)
        for j in range(n):
            mine[j] = normed[:, j * width : (j + 1) * width]
    order = list(range(n - 1, 0, -1))
    lead = core == ntp - 1

    def row_copy(d):
        peer = flipped(me, d)
        return remote(mine.at[peer], cells.at[me], xs.at[d - 1, 0], xr.at[d - 1], "fs", peer)

    def pass_copy(d, e):
        at = cells.at[flipped(me, d)]
        return remote(at, at, xs.at[d - 1, 1 + e], xr.at[d - 1], "tp", e)

    with jax.named_scope("barrier"):

        @pl.when(lead)
        def _():
            pl.semaphore_wait(pltpu.get_barrier_semaphore(), count)
            for d in order:
                row_copy(d).start()

    with jax.named_scope("latent"):
        for load in loads[2:4]:
            load.wait()
        dl_ref, rl_ref = lowers
        decay = jnp.zeros((x.shape[0], dl_ref.shape[1]), f32)
        rate = jnp.zeros((x.shape[0], rl_ref.shape[1]), f32)
        for j in range(n):
            block = mine[j]
            decay = decay + dot(block, dl_ref[j * width : (j + 1) * width])
            rate = rate + dot(block, rl_ref[j * width : (j + 1) * width])
        lat_ref[0] = jnp.tanh(decay.astype(bf16).astype(f32)).astype(bf16)
        lat_ref[1] = rate.astype(bf16)
        for load in loads[4:]:
            load.wait()
    with jax.named_scope("xwait"):
        @pl.when(lead)
        def _():
            for d in order:
                row_copy(d).wait_recv()
                for e in range(ntp - 1):
                    pass_copy(d, e).start()

        @pl.when(jnp.logical_not(lead))
        def _():
            for d in order:
                pass_copy(d, 0).wait_recv()

        greet_line()

    first, second, across = routes(me, n, core)
    targets = (first, across)

    def span_of(g):
        at, count = plan[g]
        return pl.ds(at, count)

    def first_copy(g, slot):
        return remote(
            part.at[slot, span_of(g)],
            landed.at[slot, span_of(g)],
            loaded.at[2 * g + slot],
            pr.at[g, slot],
            "fs",
            first,
        )

    def first_pool(slot):
        return remote(
            pool_part.at[slot],
            pool_landed.at[slot],
            loaded.at[2 * groups + slot],
            pr.at[groups, slot],
            "fs",
            first,
        )

    def second_copy(g):
        return remote(
            onward.at[span_of(g)], joined.at[span_of(g)], loaded.at[2 * groups + 2 + g], qr.at[g], "fs", second
        )

    second_pool = remote(
        pool_onward, pool_joined, loaded.at[3 * groups + 2], qr.at[groups], "fs", second
    )

    def piece(m, g):
        at, count = plan[g]
        return weights[m][:, at * LANES : (at + count) * LANES]

    def beside(ref, g, m):
        at, count = plan[g]
        return jnp.concatenate([ref[p, m] for p in range(at, at + count)], 1).astype(f32)

    def keep(ref, g, m, cells):
        at, count = plan[g]
        for j in range(count):
            ref[at + j, m] = cells[:, j * LANES : (j + 1) * LANES].astype(bf16)

    with jax.named_scope("partials"):
        for g in range(groups):
            for slot in (1, 0):
                for m in range(3):
                    keep(part.at[slot], g, m, dot(cells[targets[slot]], piece(m, g)))
                first_copy(g, slot).start()

    def forward(g):
        with jax.named_scope(f"fwd{g}"):
            terms = [dot(cells[second], piece(m, g)) for m in range(3)]
            first_copy(g, 1).wait_recv()
            for m in range(3):
                keep(onward, g, m, terms[m] + beside(landed.at[1], g, m))
            second_copy(g).start()

    def ready_pool():
        with jax.named_scope("readypool"):
            for slot in (1, 0):
                pool_part[slot] = dot(cells[targets[slot]], weights[3][...]).astype(bf16)
            own_rims(lambda rows: dot(mine[me, rows], weights[3][...]))

    def begin_pool():
        with jax.named_scope("beginpool"):
            send_rims(1, pool_part.at[0], first)
            for slot in (1, 0):
                first_pool(slot).start()

    def forward_pool():
        with jax.named_scope("fwdpool"):
            term = dot(cells[second], weights[3][...])
            first_pool(1).wait_recv()
            pool_onward[...] = (term + pool_landed[1].astype(f32)).astype(bf16)
            send_rims(2, pool_onward, second)
            second_pool.start()

    def prep(g):
        with jax.named_scope(f"prep{g}"):
            prepare(g)
            at, count = plan[g]
            for m in range(3):
                term = dot(mine[me], piece(m, g))
                for j in range(count):
                    own_part[at + j, m] = term[:, j * LANES : (j + 1) * LANES]

    def settle(g):
        with jax.named_scope(f"settle{g}"):
            first_copy(g, 0).wait_recv()
            second_copy(g).wait_recv()
        with jax.named_scope(f"mix{g}"):
            owned = [
                (
                    beside(own_part, g, m)
                    + beside(landed.at[0], g, m)
                    + beside(joined, g, m)
                ).astype(bf16)
                for m in range(3)
            ]
            mix_group(g, *owned)

    prep(0)
    forward(0)
    prep(1)
    prep(2)
    forward(1)
    meet_line()
    settle(0)
    ready_pool()
    forward(2)
    begin_pool()
    settle(1)
    forward_pool()
    settle(2)
    def settle_pool():
        with jax.named_scope("poolin"):
            term = dot(mine[me], weights[3][...])
            first_pool(0).wait_recv()
            second_pool.wait_recv()
            pool_ref[...] = (
                term
                + pool_landed[0].astype(f32)
                + pool_joined[...].astype(f32)
            ).astype(bf16)

    def finish():
        @pl.when(lead)
        def _():
            for d in order:
                row_copy(d).wait_send()
                for e in range(ntp - 1):
                    pass_copy(d, e).wait_send()

    def free_sends():
        for g in range(groups):
            for slot in (1, 0):
                first_copy(g, slot).wait_send()
            second_copy(g).wait_send()
        for slot in (1, 0):
            first_pool(slot).wait_send()
        second_pool.wait_send()

    return free_sends, settle_pool, finish


def group_plan(pairs):
    quarter = pairs // 4
    return [(0, quarter), (quarter, pairs - 2 * quarter), (pairs - quarter, quarter)]


def routes(me, n, core):
    low, high = flipped(me, 1), flipped(me, n // 2)
    odd = lax.rem(core, 2)
    return low + odd * (high - low), high + odd * (low - high), flipped(me, n // 2 + 1)


def cut(cells, j):
    return cells[:, j * LANES : (j + 1) * LANES]


def live_rows(d, i, tokens):
    return slice(0, (i + 1) * BLOCK) if d == 0 else slice(i * BLOCK, tokens)


def prepare_group(
    start,
    per,
    lat_ref,
    draise_ref,
    dbias_ref,
    rraise_ref,
    rbias_ref,
    tempo_ref,
    extra_ref,
    fade_ref,
    grow_ref,
):
    tokens = lat_ref.shape[1]
    wide = per * LANES
    lanes = slice(start * LANES, start * LANES + wide)
    lane = lax.broadcasted_iota(jnp.int32, (tokens, LANES), 1)
    row = lax.broadcasted_iota(jnp.int32, (tokens, LANES), 0)
    head0 = lane < HEAD
    heads = tempo_ref.shape[1]
    spread = (
        lax.broadcasted_iota(jnp.int32, (heads, wide), 0)
        == 2 * start + lax.broadcasted_iota(jnp.int32, (heads, wide), 1) // HEAD
    ).astype(f32)
    spread = jnp.concatenate([spread] * 3, 0)

    def spread_out(cells):
        return dot_cols(jnp.concatenate(split_exact(cells, 3), 0), spread)

    blocks = tokens // BLOCK
    zero_row = jnp.zeros((1, wide), f32)
    for d in range(2):
        lat_mask = head0 if d == 0 else ~head0
        lat_d = jnp.where(lat_mask, lat_ref[0].astype(f32), 0.0)
        lat_r = jnp.where(lat_mask, lat_ref[1].astype(f32), 0.0)
        pre = dbias_ref[d : d + 1, lanes] + dot(lat_d, draise_ref[:, lanes])
        velocity = jax.nn.sigmoid(pre) * 0.6065306597126334
        ld = -velocity * spread_out(tempo_ref[d]) + spread_out(extra_ref[d])
        rate = jax.nn.sigmoid(rbias_ref[d : d + 1, lanes] + dot(lat_r, rraise_ref[:, lanes]))
        upto = (lane <= row) if d == 0 else (lane >= row)
        tri = upto.astype(f32).astype(bf16)
        inner = dot(jnp.concatenate([tri, tri], 1), jnp.concatenate(split_exact(ld, 2), 0))
        excl = inner - ld
        last = inner[tokens - 1 : tokens] if d == 0 else inner[0:1]
        fade_ref[d, 0, :, lanes] = jnp.exp(excl)
        fade_ref[d, 1, :, lanes] = jnp.exp(inner)
        fade_ref[d, 2, :, lanes] = jnp.exp(last - inner) * rate
        for i in range(blocks):
            lo, hi = i * BLOCK, (i + 1) * BLOCK
            if d == 0:
                base = inner[lo - 1 : lo] if i > 0 else zero_row
            else:
                base = inner[hi : hi + 1] if i < blocks - 1 else zero_row
            live = live_rows(d, i, tokens)
            fade_ref[d, 3, lo:hi, lanes] = jnp.exp(excl[lo:hi] - base)
            fade_ref[d, 4, lo:hi, lanes] = jnp.exp(inner[lo:hi] - base)
            grow = jnp.exp(jnp.minimum(base - inner[live], 80.0))
            grow_ref[d, i, live, lanes] = grow * rate[live]


def mix_group(
    start,
    key,
    receptance,
    value,
    fade_ref,
    grow_ref,
    query_ref,
    local_ref,
    transfer_ref,
    carried_ref,
):
    tokens, wide = key.shape
    per = wide // LANES
    kf = key.astype(f32)
    rf = receptance.astype(f32)
    lane = lax.broadcasted_iota(jnp.int32, (tokens, LANES), 1)
    row = lax.broadcasted_iota(jnp.int32, (tokens, LANES), 0)
    head0 = lane < HEAD
    only = [head0.astype(f32).astype(bf16), (~head0).astype(f32).astype(bf16)]
    blank = jnp.zeros((tokens, LANES), bf16)

    def both_heads(cells):
        return jnp.concatenate([cells * only[0], cells * only[1]], 0)

    def rows_for_heads(cells):
        return jnp.concatenate(
            [jnp.concatenate([cut(cells, i) * o for i in range(cells.shape[1] // LANES)], 1) for o in only], 0
        )

    units = []
    for j in range(per):
        kj = cut(kf, j)
        k2 = kj * kj
        s0 = jnp.sum(jnp.where(head0, k2, 0.0), axis=-1, keepdims=True)
        s1 = jnp.sum(jnp.where(head0, 0.0, k2), axis=-1, keepdims=True)
        units.append(kj * lax.rsqrt(jnp.where(head0, s0, s1) + unit_eps))
    blocks = tokens // BLOCK
    eye = (row == lane).astype(f32)
    sizes = []
    size = 1
    while size < tokens:
        sizes.append(size)
        size *= 2

    def level_mask(k):
        return ((row >> (k + 1)) == (lane >> (k + 1))) & ((row >> k) != (lane >> k))

    ways = [[] for _ in range(per)]
    for d in range(2):
        upto = (lane <= row) if d == 0 else (lane >= row)
        strict = (lane < row) if d == 0 else (lane > row)
        for j in range(per):
            at = slice((start + j) * LANES, (start + j + 1) * LANES)
            unit, kj, rj = units[j], cut(kf, j), cut(rf, j)
            aheads = unit * fade_ref[d, 3, :, at]
            queries = rj * fade_ref[d, 4, :, at]
            firsts = [
                jnp.where(head0, aheads, 0.0).astype(bf16),
                jnp.where(head0, 0.0, aheads).astype(bf16),
                jnp.where(head0, queries, 0.0).astype(bf16),
                jnp.where(head0, 0.0, queries).astype(bf16),
            ]
            grams = []
            for i in range(blocks):
                lo, hi = i * BLOCK, (i + 1) * BLOCK
                live = live_rows(d, i, tokens)
                grow = grow_ref[d, i, live, at]
                rest = tokens - grow.shape[0]

                def filled(cells):
                    cells = cells.astype(bf16)
                    if not rest:
                        return cells
                    empty = jnp.zeros((rest, LANES), bf16)
                    return jnp.concatenate([cells, empty] if d == 0 else [empty, cells], 0)

                right = jnp.concatenate(
                    [filled(unit[live] * grow), filled(kj[live] * grow)], 0
                )
                grams.append(dot_rows(jnp.concatenate([f[lo:hi] for f in firsts], 0), right))

            def gathered(place, at, mask):
                rows = jnp.concatenate(
                    [
                        gram[place * BLOCK : (place + 1) * BLOCK, at * tokens : (at + 1) * tokens]
                        for gram in grams
                    ],
                    0,
                )
                return jnp.where(mask, rows, 0.0)

            way = dict()
            way["link"] = [gathered(h, 0, strict) for h in range(2)]
            way["write"] = [gathered(h, 1, strict).astype(bf16) for h in range(2)]
            way["read"] = [gathered(2 + h, 0, upto).astype(bf16) for h in range(2)]
            way["read_write"] = [gathered(2 + h, 1, upto).astype(bf16) for h in range(2)]
            ways[j].append(way)

    links = [link for j in range(per) for way in ways[j] for link in way["link"]]
    mask = level_mask(0)
    inverses = [(eye - jnp.where(mask, a, 0.0)).astype(bf16) for a in links]
    links = [a.astype(bf16) for a in links]

    def products(lefts, rights):
        out = []
        for i in range(0, len(lefts), 2):
            result = dot(
                jnp.concatenate(lefts[i : i + 2], 1),
                jnp.concatenate(
                    [
                        jnp.concatenate([rights[i], blank], 1),
                        jnp.concatenate([blank, rights[i + 1]], 1),
                    ],
                    0,
                ),
            ).astype(bf16)
            out += [cut(result, 0), cut(result, 1)]
        return out

    def level_bits(k):
        return level_mask(k).astype(f32).astype(bf16)

    for k in range(1, len(sizes), 2):
        if k + 1 == len(sizes):
            mask = level_bits(k)
            firsts = products(inverses, [a * mask for a in links])
            steps = products(firsts, inverses)
            inverses = [t - u for t, u in zip(inverses, steps)]
            continue
        mask = level_bits(k) + level_bits(k + 1)
        firsts = products(inverses, [a * mask for a in links])
        steps = products(firsts, inverses)
        squares = products(firsts, firsts)
        inverses = [t - u for t, u in zip(inverses, steps)]
        inverses = [t + u for t, u in zip(inverses, products(squares, inverses))]

    block_diag = (row < HEAD) == head0
    for j in range(per):
        pair = start + j
        vj = cut(value, j)
        stacked = both_heads(vj)
        sums = dot(
            jnp.concatenate(
                [
                    jnp.concatenate(way[name], 1)
                    for way in ways[j]
                    for name in ("write", "read_write")
                ],
                0,
            ),
            stacked,
        )
        local = sums[tokens : 2 * tokens] + sums[3 * tokens :]
        at = slice(pair * LANES, (pair + 1) * LANES)
        for d, way in enumerate(ways[j]):
            ahead = units[j] * fade_ref[d, 0, :, at]
            query = cut(rf, j) * fade_ref[d, 1, :, at]
            edge_row = tokens - 1 if d == 0 else 0
            last = fade_ref[d, 1, edge_row : edge_row + 1, at]
            base = sums[2 * d * tokens : (2 * d + 1) * tokens]
            rhs = jnp.concatenate([ahead.astype(bf16), base.astype(bf16)], 1)
            place = 4 * j + 2 * d
            solved = -dot(jnp.concatenate(inverses[place : place + 2], 1), rows_for_heads(rhs))
            solved = solved.astype(bf16)
            tail = fade_ref[d, 2, :, at]
            remove_tail = (units[j] * tail).astype(bf16)
            write_tail = (cut(kf, j) * tail).astype(bf16)
            seen = dot(jnp.concatenate(way["read"], 1), rows_for_heads(solved))
            query_ref[d, :, pair * LANES : (pair + 1) * LANES] = (query + cut(seen, 0)).astype(bf16)
            local = local + cut(seen, 1)
            onto = dot_cols(remove_tail, solved)
            transfer = jnp.where(block_diag, cut(onto, 0), 0.0) + eye * last
            transfer_ref[d, pair] = transfer.astype(bf16)
            carried = cut(onto, 1) + dot_cols(write_tail, vj)
            carried_ref[d, pair] = jnp.where(
                head0[:HEAD], carried[:HEAD], carried[HEAD:]
            )
        local_ref[:, pair * LANES : (pair + 1) * LANES] = local


def layer_kernel(
    nsp,
    nfs,
    ntp,
    x_hbm,
    in_gain_hbm,
    wk_hbm,
    wr_hbm,
    wv_hbm,
    wi_hbm,
    dl_hbm,
    rl_hbm,
    draise_hbm,
    dbias_hbm,
    rraise_hbm,
    rbias_hbm,
    tempo_hbm,
    extra_hbm,
    mix_hbm,
    gain_hbm,
    wa_hbm,
    wp_hbm,
    out_hbm,
    x_ref,
    in_gain_ref,
    draise_ref,
    dbias_ref,
    rraise_ref,
    rbias_ref,
    tempo_ref,
    extra_ref,
    gain_ref,
    wk_ref,
    wr_ref,
    wv_ref,
    wi_ref,
    dl_ref,
    rl_ref,
    mix_ref,
    wa_ref,
    wp_ref,
    loaded,
    mine,
    cells,
    part,
    pool_part,
    own_part,
    onward,
    pool_onward,
    landed,
    pool_landed,
    joined,
    pool_joined,
    xs,
    xr,
    ready,
    pr,
    qr,
    lat_ref,
    fade_ref,
    grow_ref,
    pool_ref,
    query_ref,
    local_ref,
    transfer_ref,
    carried_ref,
    edge,
    halo,
    rims,
    incoming,
    leaving,
    near_state,
    near_map,
    skipped,
    onto_next,
    act,
    tsend,
    trecv,
    sums_ref,
    osend,
    hs,
    hr,
    ss,
    sr,
    gr,
    ts,
    tr,
    os,
    orr,
):
    z = lax.axis_index("sp")
    me = lax.axis_index("fs")
    core = lax.axis_index("tp")
    tokens, channels = local_ref.shape
    depth = wa_ref.shape[0]
    half_rows = tokens // ntp
    has_prev = z > 0
    has_next = z < nsp - 1
    prev = jnp.maximum(z - 1, 0)
    after = jnp.minimum(z + 1, nsp - 1)
    prev2 = jnp.maximum(z - 2, 0)
    after2 = jnp.minimum(z + 2, nsp - 1)

    barrier = pltpu.get_barrier_semaphore()
    lead = core == ntp - 1

    @pl.when(lead)
    def _():
        for d in range(1, nfs):
            greet(barrier, "fs", flipped(me, d))

    @pl.when(jnp.logical_not(lead))
    def _():
        greet(barrier, "tp", ntp - 1)

    near = ((has_prev, prev), (has_next, after), (z > 1, prev2), (z < nsp - 2, after2))

    def greet_line():
        @pl.when(core == 0)
        def _():
            for there, peer in near:
                pl.when(there)(lambda: greet(barrier, "sp", peer))

    def meet_line():
        @pl.when(core == 0)
        def _():
            count = 0
            for there, _ in near:
                count = count + jnp.where(there, 1, 0)
            pl.semaphore_wait(barrier, count)
            for e in range(1, ntp):
                greet(ready, "tp", e)

        @pl.when(core != 0)
        def _():
            pl.semaphore_wait(ready, 1)

    small = (draise_hbm, dbias_hbm, rraise_hbm, rbias_hbm, tempo_hbm, extra_hbm, gain_hbm)
    sources = (x_hbm, in_gain_hbm, dl_hbm, rl_hbm, wk_hbm, wr_hbm, wv_hbm, wi_hbm)
    sources += small + (mix_hbm, wa_hbm, wp_hbm)
    small = (draise_ref, dbias_ref, rraise_ref, rbias_ref, tempo_ref, extra_ref, gain_ref)
    targets = (x_ref, in_gain_ref, dl_ref, rl_ref, wk_ref, wr_ref, wv_ref, wi_ref)
    targets += small + (mix_ref, wa_ref, wp_ref)
    loads = [
        pltpu.make_async_copy(source, target, loaded.at[i])
        for i, (source, target) in enumerate(zip(sources, targets))
    ]
    for load in loads:
        load.start()
    plan = group_plan(transfer_ref.shape[1])
    groups = len(plan)

    STATE, NEAR, MAP, SKIP = range(4)
    places = (z, nsp - 1 - z)
    odd = [lax.rem(place, 2) == 1 for place in places]

    def both(*tests):
        result = tests[0]
        for test in tests[1:]:
            result = jnp.logical_and(result, test)
        return result

    def state_copy(kind, d, g):
        span = pl.ds(plan[g][0], plan[g][1])
        source = (onto_next, leaving, transfer_ref, onto_next)[kind]
        target = (incoming, near_state, near_map, skipped)[kind]
        step = (after, prev) if kind != SKIP else (after2, prev2)
        return remote(
            source.at[d, span],
            target.at[d, span],
            ss.at[(0, 0, 1, 1)[kind], d, g],
            sr.at[(0, 0, 1, 2)[kind], d, g],
            "sp",
            step[d],
        )

    def starts(d):
        place = places[d]
        goes = place < nsp - 1
        return (
            (STATE, both(odd[d], goes)),
            (NEAR, both(jnp.logical_not(odd[d]), goes)),
            (MAP, both(jnp.logical_not(odd[d]), goes, place > 0)),
            (SKIP, both(odd[d], place < nsp - 2)),
        )

    ends = (pl.ds(tokens - HALO, HALO), pl.ds(0, HALO))

    def rim_copy(c, d, source, owner):
        return pltpu.make_async_remote_copy(
            src_ref=source,
            dst_ref=rims.at[d, c],
            send_sem=hs.at[c, d],
            recv_sem=hr.at[c, d],
            device_id={"fs": owner, "sp": after if d == 0 else prev},
            device_id_type=pl.DeviceIdType.MESH,
        )

    def send_rims(c, source, owner):
        for d in range(2):
            pl.when(sends[d])(lambda: rim_copy(c, d, source.at[ends[d]], owner).start())

    def own_rims(rows_of):
        for d in range(2):
            edge[d] = rows_of(ends[d]).astype(bf16)
            pl.when(sends[d])(lambda: rim_copy(0, d, edge.at[d], me).start())

    sends = [has_next, has_prev]
    takes = [has_prev, has_next]

    def pairs_of(g):
        return range(plan[g][0], plan[g][0] + plan[g][1])

    def mix_step(g, *operands):
        mix_group(plan[g][0], *operands)
        for d in range(2):

            @pl.when(places[d] == 0)
            def _():
                for p in pairs_of(g):
                    incoming[d, p] = jnp.zeros_like(incoming[d, p])

            for p in pairs_of(g):
                leaving[d, p] = carried_ref[d, p].astype(bf16)
            for kind, goes in starts(d)[NEAR : MAP + 1]:
                pl.when(goes)(lambda: state_copy(kind, d, g).start())

    def doubled(state):
        top0 = lax.broadcasted_iota(jnp.int32, state.shape, 1) < HEAD
        state = state.astype(f32)
        return jnp.concatenate([jnp.where(top0, state, 0.0), jnp.where(top0, 0.0, state)], 0)

    def moved(by, state):
        both_halves = dot(by, doubled(state))
        return both_halves[:HEAD] + both_halves[HEAD:]

    def relay(d, g):
        place = places[d]

        @pl.when(odd[d])
        def _():
            state_copy(NEAR, d, g).wait_recv()

            @pl.when(place == 1)
            def _():
                for p in pairs_of(g):
                    incoming[d, p] = near_state[d, p]

            @pl.when(place > 1)
            def _():
                state_copy(MAP, d, g).wait_recv()
                state_copy(SKIP, d, g).wait_recv()
                for p in pairs_of(g):
                    incoming[d, p] = (
                        moved(near_map[d, p], skipped[d, p]) + near_state[d, p].astype(f32)
                    ).astype(bf16)

            @pl.when(place < nsp - 1)
            def _():
                for p in pairs_of(g):
                    onto_next[d, p] = (
                        moved(transfer_ref[d, p], incoming[d, p]) + carried_ref[d, p]
                    ).astype(bf16)
                state_copy(STATE, d, g).start()
                pl.when(place < nsp - 2)(lambda: state_copy(SKIP, d, g).start())

        @pl.when(both(jnp.logical_not(odd[d]), place > 0))
        def _():
            state_copy(STATE, d, g).wait_recv()

    early = 2 * z < nsp

    def relays(near, g):
        @pl.when(early)
        def _():
            relay(0 if near else 1, g)

        @pl.when(jnp.logical_not(early))
        def _():
            relay(1 if near else 0, g)

    free_sends, settle_pool, finish_front = front_part(
        nfs,
        x_ref,
        in_gain_ref,
        (wk_ref, wr_ref, wv_ref, wi_ref),
        (dl_ref, rl_ref),
        loads[:15],
        pool_ref,
        lat_ref,
        mine,
        cells,
        part,
        pool_part,
        own_part,
        onward,
        pool_onward,
        landed,
        pool_landed,
        joined,
        pool_joined,
        xs,
        xr,
        loaded,
        pr,
        qr,
        nfs + ntp - 2,
        greet_line,
        meet_line,
        send_rims,
        own_rims,
        lambda g: prepare_group(
            plan[g][0],
            plan[g][1],
            lat_ref,
            draise_ref,
            dbias_ref,
            rraise_ref,
            rbias_ref,
            tempo_ref,
            extra_ref,
            fade_ref,
            grow_ref,
        ),
        lambda g, key, receptance, value: mix_step(
            g,
            key,
            receptance,
            value,
            fade_ref,
            grow_ref,
            query_ref,
            local_ref,
            transfer_ref,
            carried_ref,
        ),
    )
    for load in loads[15:]:
        load.wait()
    first, second, across = routes(me, nfs, core)

    def act_part(seq, k):
        if k == 0:
            return act.at[seq, 0]
        at, count = plan[k - 1]
        return act.at[seq, 1, :, pl.ds(at * LANES, count * LANES)]

    def share(k, seq, way, peer):
        return remote(
            act_part(seq, k), act_part(seq, k), loaded.at[3 * k + way], gr.at[k, way], "fs", peer
        )

    whole_way = groups

    def share_out(k):
        if k == whole_way:
            share(k, me, 2, across).start()
        share(k, me, 0, first).start()
        share(k, me, 1, second).start()

    def pass_on(k):
        share(k, first, 0, first).wait_recv()
        if k != whole_way:
            share(k, first, 2, second).start()

    head0 = lax.broadcasted_iota(jnp.int32, (tokens, LANES), 1) < HEAD

    def head_mean(values):
        low = jnp.sum(jnp.where(head0, values, 0.0), axis=-1, keepdims=True)
        high = jnp.sum(jnp.where(head0, 0.0, values), axis=-1, keepdims=True)
        return jnp.where(head0, low, high) * (1.0 / HEAD)

    def finish_group(g):
        with jax.named_scope(f"relayB{g}"):
            relays(False, g)
        with jax.named_scope(f"readout{g}"):
            for p in pairs_of(g):
                lanes = slice(p * LANES, (p + 1) * LANES)
                readout = local_ref[:, lanes]
                for d in range(2):
                    readout = readout + dot(query_ref[d, :, lanes], doubled(incoming[d, p]))
                centred = readout - head_mean(readout)
                scaled = centred * lax.rsqrt(head_mean(centred * centred) + head_eps)
                act[me, 1, :, lanes] = (
                    scaled * gain_ref[lanes].astype(f32).reshape(1, -1)
                ).astype(bf16)
            share_out(1 + g)

    for g in range(groups - 1):
        with jax.named_scope(f"relayA{g}"):
            relays(True, g)
    free_sends()
    settle_pool()
    with jax.named_scope("halo"):
        for d in range(2):

            @pl.when(takes[d])
            def _():
                for c in range(3):
                    rim_copy(c, d, edge.at[d], me).wait_recv()
                halo[d] = sum(rims[d, c].astype(f32) for c in range(3)).astype(bf16)

            @pl.when(jnp.logical_not(takes[d]))
            def _():
                halo[d] = jnp.zeros_like(halo[d])

    span = tokens + 2 * HALO
    rim = jnp.concatenate([halo[0], pool_ref[...], halo[1]], 0)
    here = lax.broadcasted_iota(jnp.int32, (tokens, span), 0)
    there = lax.broadcasted_iota(jnp.int32, (tokens, span), 1) - HALO
    position = z * tokens + lax.broadcasted_iota(jnp.int32, (tokens, GROUP_WIDTH), 0)
    length = tokens * nsp
    groups_here = channels // GROUP_WIDTH
    for member in range(groups_here):
        cols = slice(member * GROUP_WIDTH, (member + 1) * GROUP_WIDTH)
        reach = jnp.left_shift(1, core * groups_here + member)
        window = jnp.where((there >= here - reach) & (there < here + reach), 1.0, 0.0)
        total = dot(window, rim[:, cols])
        size = (
            jnp.minimum(position + reach, length) - jnp.maximum(position - reach, 0)
        ).astype(f32)
        diff = (total / size - pool_ref[:, cols].astype(f32)).astype(bf16)
        act[me, 0, :, cols] = dot(diff, mix_ref[member]).astype(bf16)
    share_out(0)

    with jax.named_scope("relayAlast"):
        relays(True, groups - 1)
    for g in range(groups - 1):
        finish_group(g)
    finish_group(groups - 1)

    other = lax.rem(core + 1, ntp)
    mine_at = pl.multiple_of(core * half_rows, half_rows)
    other_at = pl.multiple_of(other * half_rows, half_rows)

    def product(seq, k):
        if k == 0:
            return dot_rows(act[seq, 0], wp_ref[...])
        at, count = plan[k - 1]
        cols = slice(at * LANES, (at + count) * LANES)
        return dot_rows(act[seq, 1, :, cols], wa_ref[:, cols])

    def swap_of(i):
        return remote(tsend.at[i], trecv.at[i], ts.at[i], tr.at[i], "tp", other)

    def offer(i, total):
        sums_ref[i] = total
        tsend[i] = sums_ref[i, pl.ds(other_at, half_rows)].astype(bf16)
        swap_of(i).start()

    place = out_hbm.at[0, :, pl.ds(pl.multiple_of(me * depth, depth), depth)]

    def back(i, seq):
        return remote(osend.at[i], place, os.at[i], orr.at[i], "fs", seq)

    own_out = pltpu.make_async_copy(osend.at[0], place, os.at[0])

    def settle_out(i, seq):
        swap_of(i).wait_recv()
        osend[i] = (
            sums_ref[i, pl.ds(mine_at, half_rows)] + trecv[i].astype(f32)
        ).astype(bf16)
        (back(i, seq) if i else own_out).start()

    with jax.named_scope("prodown"):
        offer(0, sum(product(me, k) for k in range(1 + groups)))
    peers = ((1, flipped(me, 1)), (2, flipped(me, nfs // 2)), (3, across))
    turn = list(range(groups))
    for k in turn:
        with jax.named_scope(f"pass{k}"):
            pass_on(k)
            share(k, second, 1, second).wait_recv()
        with jax.named_scope(f"prod{k}"):
            for i, seq in peers[:2]:
                sums_ref[i] = product(seq, k) + (sums_ref[i] if k != turn[0] else 0.0)
        if k == turn[0]:
            settle_out(0, me)
    k = groups
    with jax.named_scope(f"wait{k}1"):
        share(k, first, 0, first).wait_recv()
        share(k, second, 1, second).wait_recv()
    for i, seq in peers[:2]:
        with jax.named_scope(f"prod{k}{i}"):
            offer(i, product(seq, k) + sums_ref[i])
    for k in turn + [groups]:
        with jax.named_scope(f"wait{k}3"):
            share(k, across, 2, across).wait_recv()
        with jax.named_scope(f"prod{k}3"):
            total = product(across, k) + (sums_ref[3] if k != turn[0] else 0.0)
            if k < groups:
                sums_ref[3] = total
            else:
                offer(3, total)
        if k == turn[0]:
            for i, seq in peers[:2]:
                with jax.named_scope(f"swapwait{i}"):
                    settle_out(i, seq)
    with jax.named_scope("swapwait3"):
        settle_out(3, across)
    with jax.named_scope("sent"):
        own_out.wait()
        for k in range(1 + groups):
            for way in range(3):
                share(k, me, way, first).wait_send()
        for i in range(1 + len(peers)):
            swap_of(i).wait_send()
        for i, seq in peers:
            back(i, seq).wait_send()
        for d in range(2):

            @pl.when(sends[d])
            def _():
                for c in range(3):
                    rim_copy(c, d, edge.at[d], me).wait_send()

            for kind, goes in starts(d):

                @pl.when(goes)
                def _():
                    for g in range(groups):
                        state_copy(kind, d, g).wait_send()
        finish_front()
    with jax.named_scope("retwait"):
        for i, seq in peers:
            back(i, seq).wait_recv()


def shards(
    inputs,
    input_norm_gain,
    receptance_matrix,
    key_matrix,
    value_matrix,
    pooling_input_weight,
    decay_lower_matrix,
    decay_raise_matrix,
    decay_offset_bias,
    removal_lower_matrix,
    removal_raise_matrix,
    removal_rate_bias,
    tempo_scale,
    sudden_decay_extra,
    head_norm_gain,
    group_mixing_weight,
    attention_output_matrix,
    pooling_output_matrix,
):
    nsp, nfs, ntp = lax.axis_size("sp"), lax.axis_size("fs"), lax.axis_size("tp")
    _, tokens, features = inputs.shape
    depth, channels = key_matrix.shape
    pairs = channels // LANES
    groups = len(group_plan(pairs))
    dma = pltpu.SemaphoreType.DMA
    rank = decay_lower_matrix.shape[1]
    rank2 = decay_raise_matrix.shape[0] * decay_raise_matrix.shape[1]
    anywhere = pl.BlockSpec(memory_space=pl.ANY)
    half = (nfs, tokens // ntp, depth)
    return pl.pallas_call(
        functools.partial(layer_kernel, nsp, nfs, ntp),
        out_shape=pltpu.VMEM((1, tokens // ntp, features), bf16),
        in_specs=[anywhere] * 18,
        out_specs=anywhere,
        scratch_shapes=[
            pltpu.VMEM(inputs.shape, bf16),
            pltpu.VMEM(input_norm_gain.shape, bf16),
            pltpu.VMEM((rank2, channels), bf16),
            pltpu.VMEM(decay_offset_bias.shape, f32),
            pltpu.VMEM((rank2, channels), bf16),
            pltpu.VMEM(removal_rate_bias.shape, f32),
            pltpu.VMEM(tempo_scale.shape[1:], f32),
            pltpu.VMEM(sudden_decay_extra.shape[1:], f32),
            pltpu.VMEM(head_norm_gain.shape, bf16),
        ]
        + [pltpu.VMEM((depth, channels), bf16)] * 4
        + [
            pltpu.VMEM((features, rank), bf16),
            pltpu.VMEM((features, rank), bf16),
            pltpu.VMEM(group_mixing_weight.shape, bf16),
            pltpu.VMEM(attention_output_matrix.shape, bf16),
            pltpu.VMEM(pooling_output_matrix.shape, bf16),
            dma((18,)),
            pltpu.VMEM((nfs, tokens, depth), bf16),
            pltpu.VMEM((nfs, tokens, depth), bf16),
            pltpu.VMEM((2, pairs, 3, tokens, LANES), bf16),
            pltpu.VMEM((2, tokens, channels), bf16),
            pltpu.VMEM((pairs, 3, tokens, LANES), f32),
            pltpu.VMEM((pairs, 3, tokens, LANES), bf16),
            pltpu.VMEM((tokens, channels), bf16),
            pltpu.VMEM((2, pairs, 3, tokens, LANES), bf16),
            pltpu.VMEM((2, tokens, channels), bf16),
            pltpu.VMEM((pairs, 3, tokens, LANES), bf16),
            pltpu.VMEM((tokens, channels), bf16),
            dma((nfs - 1, ntp)),
            dma((nfs - 1,)),
            pltpu.SemaphoreType.REGULAR,
            dma((groups + 1, 2)),
            dma((groups + 1,)),
            pltpu.VMEM((2, tokens, rank), bf16),
            pltpu.VMEM((2, 5, tokens, channels), f32),
            pltpu.VMEM((2, tokens // BLOCK, tokens, channels), f32),
            pltpu.VMEM((tokens, channels), bf16),
            pltpu.VMEM((2, tokens, channels), bf16),
            pltpu.VMEM((tokens, channels), f32),
            pltpu.VMEM((2, pairs, LANES, LANES), bf16),
            pltpu.VMEM((2, pairs, HEAD, LANES), f32),
            pltpu.VMEM((2, HALO, channels), bf16),
            pltpu.VMEM((2, HALO, channels), bf16),
            pltpu.VMEM((2, 3, HALO, channels), bf16),
            pltpu.VMEM((2, pairs, HEAD, LANES), bf16),
            pltpu.VMEM((2, pairs, HEAD, LANES), bf16),
            pltpu.VMEM((2, pairs, HEAD, LANES), bf16),
            pltpu.VMEM((2, pairs, LANES, LANES), bf16),
            pltpu.VMEM((2, pairs, HEAD, LANES), bf16),
            pltpu.VMEM((2, pairs, HEAD, LANES), bf16),
            pltpu.VMEM((nfs, 2, tokens, channels), bf16),
            pltpu.VMEM(half, bf16),
            pltpu.VMEM(half, bf16),
            pltpu.VMEM((nfs, tokens, depth), f32),
            pltpu.VMEM(half, bf16),
            dma((3, 2)),
            dma((3, 2)),
            dma((2, 2, groups)),
            dma((3, 2, groups)),
            dma((1 + groups, 3)),
            dma((nfs,)),
            dma((nfs,)),
            dma((nfs,)),
            dma((nfs,)),
        ],
        compiler_params=pltpu.CompilerParams(
            collective_id=0, has_side_effects=True, vmem_limit_bytes=60 * 1024 * 1024
        ),
        name="layer",
    )(
        inputs,
        input_norm_gain,
        key_matrix,
        receptance_matrix,
        value_matrix,
        pooling_input_weight,
        decay_lower_matrix,
        removal_lower_matrix,
        decay_raise_matrix.reshape(rank2, channels),
        decay_offset_bias,
        removal_raise_matrix.reshape(rank2, channels),
        removal_rate_bias,
        tempo_scale[0],
        sudden_decay_extra[0],
        group_mixing_weight,
        head_norm_gain,
        attention_output_matrix,
        pooling_output_matrix,
    )


def solution(mesh):
    in_specs = (
        P("fs", "sp", None),
        P(),
        P("fs", "tp"),
        P("fs", "tp"),
        P("fs", "tp"),
        P("fs", "tp"),
        P(),
        P(None, None, "tp"),
        P(None, "tp"),
        P(),
        P(None, None, "tp"),
        P(None, "tp"),
        P("fs", None, "tp", "sp"),
        P("fs", None, "tp", "sp"),
        P("tp"),
        P("tp", None, None),
        P("fs", "tp"),
        P("fs", "tp"),
    )
    out_specs = P("fs", ("sp", "tp"), None)
    return jax.shard_map(shards, mesh=mesh, in_specs=in_specs, out_specs=out_specs, check_vma=False)
```

```python
import functools

import jax
import jax.numpy as jnp
from jax import lax
from jax.experimental import pallas as pl
from jax.experimental.pallas import tpu as pltpu
from jax.sharding import PartitionSpec as P

HEAD = 64
GROUP_WIDTH = 256
LANES = 128
BLOCK = 16
HALO = 16

norm_eps = 1e-06
head_eps = 0.00064
unit_eps = 1e-06
f32 = jnp.float32
bf16 = jnp.bfloat16
VMEM = pl.BlockSpec(memory_space=pltpu.VMEM)


def dot(left, right):
    return jnp.dot(left.astype(bf16), right.astype(bf16), preferred_element_type=f32)


def dot_general(left, right, dims):
    return lax.dot_general(
        left.astype(bf16), right.astype(bf16), (dims, ((), ())), preferred_element_type=f32
    )


def dot_rows(left, right):
    return dot_general(left, right, ((1,), (1,)))


def dot_cols(left, right):
    return dot_general(left, right, ((0,), (0,)))


def split_exact(cells, pieces):
    parts = []
    for _ in range(pieces - 1):
        high = cells.astype(bf16).astype(f32)
        parts.append(high)
        cells = cells - high
    return parts + [cells]


def remote(src, dst, send, recv, axis, peer):
    return pltpu.make_async_remote_copy(
        src_ref=src,
        dst_ref=dst,
        send_sem=send,
        recv_sem=recv,
        device_id={axis: peer},
        device_id_type=pl.DeviceIdType.MESH,
    )


def greet(barrier, axis, peer):
    pl.semaphore_signal(
        barrier, inc=1, device_id={axis: peer}, device_id_type=pl.DeviceIdType.MESH
    )


def flipped(at, bits):
    moved = at
    bit = 1
    while bit <= bits:
        if bits & bit:
            moved = moved + bit - 2 * bit * lax.rem(at // bit, 2)
        bit *= 2
    return moved


def front_part(
    n,
    x_ref,
    gain_ref,
    weights,
    lowers,
    loads,
    pool_ref,
    lat_ref,
    mine,
    cells,
    part,
    pool_part,
    own_part,
    onward,
    pool_onward,
    landed,
    pool_landed,
    joined,
    pool_joined,
    xs,
    xr,
    loaded,
    pr,
    qr,
    count,
    greet_line,
    meet_line,
    send_rims,
    own_rims,
    first_relay,
    prepare,
    mix_group,
):
    me = lax.axis_index("fs")
    core, ntp = lax.axis_index("tp"), lax.axis_size("tp")
    width = x_ref.shape[2] // n
    plan = group_plan(part.shape[1])
    groups = len(plan)
    with jax.named_scope("xload"):
        for load in loads[:2]:
            load.wait()
    x = x_ref[0].astype(f32)
    with jax.named_scope("norm"):
        normed = (
            x
            * lax.rsqrt(jnp.mean(x * x, axis=-1, keepdims=True) + norm_eps)
            * gain_ref[...].astype(f32).reshape(1, -1)
        ).astype(bf16)
        for j in range(n):
            mine[j] = normed[:, j * width : (j + 1) * width]
    order = list(range(n - 1, 0, -1))
    lead = core == ntp - 1

    def row_copy(d):
        peer = flipped(me, d)
        return remote(mine.at[peer], cells.at[me], xs.at[d - 1, 0], xr.at[d - 1], "fs", peer)

    def pass_copy(d, e):
        at = cells.at[flipped(me, d)]
        return remote(at, at, xs.at[d - 1, 1 + e], xr.at[d - 1], "tp", e)

    with jax.named_scope("barrier"):

        @pl.when(lead)
        def _():
            pl.semaphore_wait(pltpu.get_barrier_semaphore(), count)
            for d in order:
                row_copy(d).start()

    with jax.named_scope("latent"):
        for load in loads[2:4]:
            load.wait()
        dl_ref, rl_ref = lowers
        decay = jnp.zeros((x.shape[0], dl_ref.shape[1]), f32)
        rate = jnp.zeros((x.shape[0], rl_ref.shape[1]), f32)
        for j in range(n):
            block = mine[j]
            decay = decay + dot(block, dl_ref[j * width : (j + 1) * width])
            rate = rate + dot(block, rl_ref[j * width : (j + 1) * width])
        lat_ref[0] = jnp.tanh(decay.astype(bf16).astype(f32)).astype(bf16)
        lat_ref[1] = rate.astype(bf16)
        for load in loads[4:]:
            load.wait()
    with jax.named_scope("xwait"):
        @pl.when(lead)
        def _():
            for d in order:
                row_copy(d).wait_recv()
                for e in range(ntp - 1):
                    pass_copy(d, e).start()

    def meet_rows(d):
        with jax.named_scope("rows"):

            @pl.when(jnp.logical_not(lead))
            def _():
                pass_copy(d, 0).wait_recv()

    first, second, across = routes(me, n, core)
    targets = (first, across)

    def span_of(g):
        at, count = plan[g]
        return pl.ds(at, count)

    def first_copy(g, slot):
        return remote(
            part.at[slot, span_of(g)],
            landed.at[slot, span_of(g)],
            loaded.at[2 * g + slot],
            pr.at[g, slot],
            "fs",
            first,
        )

    def first_pool(slot):
        return remote(
            pool_part.at[slot],
            pool_landed.at[slot],
            loaded.at[2 * groups + slot],
            pr.at[groups, slot],
            "fs",
            first,
        )

    def second_copy(g):
        return remote(
            onward.at[span_of(g)], joined.at[span_of(g)], loaded.at[2 * groups + 2 + g], qr.at[g], "fs", second
        )

    second_pool = remote(
        pool_onward, pool_joined, loaded.at[3 * groups + 2], qr.at[groups], "fs", second
    )

    def piece(m, g):
        at, count = plan[g]
        return weights[m][:, at * LANES : (at + count) * LANES]

    def beside(ref, g, m):
        at, count = plan[g]
        return jnp.concatenate([ref[p, m] for p in range(at, at + count)], 1).astype(f32)

    def keep(ref, g, m, cells):
        at, count = plan[g]
        for j in range(count):
            ref[at + j, m] = cells[:, j * LANES : (j + 1) * LANES].astype(bf16)

    with jax.named_scope("partials"):
        for g in range(groups):
            for slot in (1, 0):
                if g == 0 and slot:
                    meet_rows(n // 2 + 1)
                for m in range(3):
                    keep(part.at[slot], g, m, dot(cells[targets[slot]], piece(m, g)))
                if g == 0 and slot:
                    meet_rows(1)
                first_copy(g, slot).start()

    def forward(g):
        with jax.named_scope(f"fwd{g}"):
            terms = [dot(cells[second], piece(m, g)) for m in range(3)]
            first_copy(g, 1).wait_recv()
            for m in range(3):
                keep(onward, g, m, terms[m] + beside(landed.at[1], g, m))
            second_copy(g).start()

    def ready_pool():
        with jax.named_scope("readypool"):
            for slot in (1, 0):
                pool_part[slot] = dot(cells[targets[slot]], weights[3][...]).astype(bf16)
            own_rims(lambda rows: dot(mine[me, rows], weights[3][...]))

    def begin_pool():
        with jax.named_scope("beginpool"):
            send_rims(1, pool_part.at[0], first)
            for slot in (1, 0):
                first_pool(slot).start()

    def forward_pool():
        with jax.named_scope("fwdpool"):
            term = dot(cells[second], weights[3][...])
            first_pool(1).wait_recv()
            pool_onward[...] = (term + pool_landed[1].astype(f32)).astype(bf16)
            send_rims(2, pool_onward, second)
            second_pool.start()

    def prep(g):
        with jax.named_scope(f"prep{g}"):
            prepare(g)
            at, count = plan[g]
            for m in range(3):
                term = dot(mine[me], piece(m, g))
                for j in range(count):
                    own_part[at + j, m] = term[:, j * LANES : (j + 1) * LANES]

    def settle(g):
        with jax.named_scope(f"settle{g}"):
            first_copy(g, 0).wait_recv()
            second_copy(g).wait_recv()
        with jax.named_scope(f"mix{g}"):
            owned = [
                (
                    beside(own_part, g, m)
                    + beside(landed.at[0], g, m)
                    + beside(joined, g, m)
                ).astype(bf16)
                for m in range(3)
            ]
            mix_group(g, *owned)

    meet_rows(n // 2)
    greet_line()
    prep(0)
    forward(0)
    prep(1)
    prep(2)
    forward(1)
    meet_line()
    settle(0)
    ready_pool()
    forward(2)
    begin_pool()
    settle(1)
    first_relay()
    forward_pool()
    settle(2)
    def settle_pool():
        with jax.named_scope("poolin"):
            term = dot(mine[me], weights[3][...])
            first_pool(0).wait_recv()
            second_pool.wait_recv()
            pool_ref[...] = (
                term
                + pool_landed[0].astype(f32)
                + pool_joined[...].astype(f32)
            ).astype(bf16)

    def finish():
        @pl.when(lead)
        def _():
            for d in order:
                row_copy(d).wait_send()
                for e in range(ntp - 1):
                    pass_copy(d, e).wait_send()

    def free_sends():
        for g in range(groups):
            for slot in (1, 0):
                first_copy(g, slot).wait_send()
            second_copy(g).wait_send()
        for slot in (1, 0):
            first_pool(slot).wait_send()
        second_pool.wait_send()

    return free_sends, settle_pool, finish


def group_plan(pairs):
    quarter = pairs // 4
    return [(0, quarter), (quarter, pairs - 2 * quarter), (pairs - quarter, quarter)]


def routes(me, n, core):
    low, high = flipped(me, 1), flipped(me, n // 2)
    odd = lax.rem(core, 2)
    return low + odd * (high - low), high + odd * (low - high), flipped(me, n // 2 + 1)


def cut(cells, j):
    return cells[:, j * LANES : (j + 1) * LANES]


def live_rows(d, i, tokens):
    return slice(0, (i + 1) * BLOCK) if d == 0 else slice(i * BLOCK, tokens)


def prepare_group(
    start,
    per,
    lat_ref,
    draise_ref,
    dbias_ref,
    rraise_ref,
    rbias_ref,
    tempo_ref,
    extra_ref,
    fade_ref,
    grow_ref,
):
    tokens = lat_ref.shape[1]
    wide = per * LANES
    lanes = slice(start * LANES, start * LANES + wide)
    lane = lax.broadcasted_iota(jnp.int32, (tokens, LANES), 1)
    row = lax.broadcasted_iota(jnp.int32, (tokens, LANES), 0)
    head0 = lane < HEAD
    heads = tempo_ref.shape[1]
    spread = (
        lax.broadcasted_iota(jnp.int32, (heads, wide), 0)
        == 2 * start + lax.broadcasted_iota(jnp.int32, (heads, wide), 1) // HEAD
    ).astype(f32)
    spread = jnp.concatenate([spread] * 3, 0)

    def spread_out(cells):
        return dot_cols(jnp.concatenate(split_exact(cells, 3), 0), spread)

    blocks = tokens // BLOCK
    zero_row = jnp.zeros((1, wide), f32)
    for d in range(2):
        lat_mask = head0 if d == 0 else ~head0
        lat_d = jnp.where(lat_mask, lat_ref[0].astype(f32), 0.0)
        lat_r = jnp.where(lat_mask, lat_ref[1].astype(f32), 0.0)
        pre = dbias_ref[d : d + 1, lanes] + dot(lat_d, draise_ref[:, lanes])
        velocity = jax.nn.sigmoid(pre) * 0.6065306597126334
        ld = -velocity * spread_out(tempo_ref[d]) + spread_out(extra_ref[d])
        rate = jax.nn.sigmoid(rbias_ref[d : d + 1, lanes] + dot(lat_r, rraise_ref[:, lanes]))
        upto = (lane <= row) if d == 0 else (lane >= row)
        tri = upto.astype(f32).astype(bf16)
        inner = dot(jnp.concatenate([tri, tri], 1), jnp.concatenate(split_exact(ld, 2), 0))
        excl = inner - ld
        last = inner[tokens - 1 : tokens] if d == 0 else inner[0:1]
        fade_ref[d, 0, :, lanes] = jnp.exp(excl)
        fade_ref[d, 1, :, lanes] = jnp.exp(inner)
        fade_ref[d, 2, :, lanes] = jnp.exp(last - inner) * rate
        for i in range(blocks):
            lo, hi = i * BLOCK, (i + 1) * BLOCK
            if d == 0:
                base = inner[lo - 1 : lo] if i > 0 else zero_row
            else:
                base = inner[hi : hi + 1] if i < blocks - 1 else zero_row
            live = live_rows(d, i, tokens)
            fade_ref[d, 3, lo:hi, lanes] = jnp.exp(excl[lo:hi] - base)
            fade_ref[d, 4, lo:hi, lanes] = jnp.exp(inner[lo:hi] - base)
            grow = jnp.exp(jnp.minimum(base - inner[live], 80.0))
            grow_ref[d, i, live, lanes] = grow * rate[live]


def mix_group(
    start,
    key,
    receptance,
    value,
    fade_ref,
    grow_ref,
    query_ref,
    local_ref,
    transfer_ref,
    carried_ref,
):
    tokens, wide = key.shape
    per = wide // LANES
    kf = key.astype(f32)
    rf = receptance.astype(f32)
    lane = lax.broadcasted_iota(jnp.int32, (tokens, LANES), 1)
    row = lax.broadcasted_iota(jnp.int32, (tokens, LANES), 0)
    head0 = lane < HEAD
    only = [head0.astype(f32).astype(bf16), (~head0).astype(f32).astype(bf16)]
    blank = jnp.zeros((tokens, LANES), bf16)

    def both_heads(cells):
        return jnp.concatenate([cells * only[0], cells * only[1]], 0)

    def rows_for_heads(cells):
        return jnp.concatenate(
            [jnp.concatenate([cut(cells, i) * o for i in range(cells.shape[1] // LANES)], 1) for o in only], 0
        )

    units = []
    for j in range(per):
        kj = cut(kf, j)
        k2 = kj * kj
        s0 = jnp.sum(jnp.where(head0, k2, 0.0), axis=-1, keepdims=True)
        s1 = jnp.sum(jnp.where(head0, 0.0, k2), axis=-1, keepdims=True)
        units.append(kj * lax.rsqrt(jnp.where(head0, s0, s1) + unit_eps))
    blocks = tokens // BLOCK
    eye = (row == lane).astype(f32)
    sizes = []
    size = 1
    while size < tokens:
        sizes.append(size)
        size *= 2

    def level_mask(k):
        return ((row >> (k + 1)) == (lane >> (k + 1))) & ((row >> k) != (lane >> k))

    ways = [[] for _ in range(per)]
    for d in range(2):
        upto = (lane <= row) if d == 0 else (lane >= row)
        strict = (lane < row) if d == 0 else (lane > row)
        for j in range(per):
            at = slice((start + j) * LANES, (start + j + 1) * LANES)
            unit, kj, rj = units[j], cut(kf, j), cut(rf, j)
            aheads = unit * fade_ref[d, 3, :, at]
            queries = rj * fade_ref[d, 4, :, at]
            firsts = [
                jnp.where(head0, aheads, 0.0).astype(bf16),
                jnp.where(head0, 0.0, aheads).astype(bf16),
                jnp.where(head0, queries, 0.0).astype(bf16),
                jnp.where(head0, 0.0, queries).astype(bf16),
            ]
            grams = []
            for i in range(blocks):
                lo, hi = i * BLOCK, (i + 1) * BLOCK
                live = live_rows(d, i, tokens)
                grow = grow_ref[d, i, live, at]
                rest = tokens - grow.shape[0]

                def filled(cells):
                    cells = cells.astype(bf16)
                    if not rest:
                        return cells
                    empty = jnp.zeros((rest, LANES), bf16)
                    return jnp.concatenate([cells, empty] if d == 0 else [empty, cells], 0)

                right = jnp.concatenate(
                    [filled(unit[live] * grow), filled(kj[live] * grow)], 0
                )
                grams.append(dot_rows(jnp.concatenate([f[lo:hi] for f in firsts], 0), right))

            def gathered(place, at, mask):
                rows = jnp.concatenate(
                    [
                        gram[place * BLOCK : (place + 1) * BLOCK, at * tokens : (at + 1) * tokens]
                        for gram in grams
                    ],
                    0,
                )
                return jnp.where(mask, rows, 0.0)

            way = dict()
            way["link"] = [gathered(h, 0, strict) for h in range(2)]
            way["write"] = [gathered(h, 1, strict).astype(bf16) for h in range(2)]
            way["read"] = [gathered(2 + h, 0, upto).astype(bf16) for h in range(2)]
            way["read_write"] = [gathered(2 + h, 1, upto).astype(bf16) for h in range(2)]
            ways[j].append(way)

    links = [link for j in range(per) for way in ways[j] for link in way["link"]]
    mask = level_mask(0)
    inverses = [(eye - jnp.where(mask, a, 0.0)).astype(bf16) for a in links]
    links = [a.astype(bf16) for a in links]

    def products(lefts, rights):
        out = []
        for i in range(0, len(lefts), 2):
            result = dot(
                jnp.concatenate(lefts[i : i + 2], 1),
                jnp.concatenate(
                    [
                        jnp.concatenate([rights[i], blank], 1),
                        jnp.concatenate([blank, rights[i + 1]], 1),
                    ],
                    0,
                ),
            ).astype(bf16)
            out += [cut(result, 0), cut(result, 1)]
        return out

    def level_bits(k):
        return level_mask(k).astype(f32).astype(bf16)

    for k in range(1, len(sizes), 2):
        if k + 1 == len(sizes):
            mask = level_bits(k)
            firsts = products(inverses, [a * mask for a in links])
            steps = products(firsts, inverses)
            inverses = [t - u for t, u in zip(inverses, steps)]
            continue
        mask = level_bits(k) + level_bits(k + 1)
        firsts = products(inverses, [a * mask for a in links])
        steps = products(firsts, inverses)
        squares = products(firsts, firsts)
        inverses = [t - u for t, u in zip(inverses, steps)]
        inverses = [t + u for t, u in zip(inverses, products(squares, inverses))]

    block_diag = (row < HEAD) == head0
    for j in range(per):
        pair = start + j
        vj = cut(value, j)
        stacked = both_heads(vj)
        sums = dot(
            jnp.concatenate(
                [
                    jnp.concatenate(way[name], 1)
                    for way in ways[j]
                    for name in ("write", "read_write")
                ],
                0,
            ),
            stacked,
        )
        local = sums[tokens : 2 * tokens] + sums[3 * tokens :]
        at = slice(pair * LANES, (pair + 1) * LANES)
        for d, way in enumerate(ways[j]):
            ahead = units[j] * fade_ref[d, 0, :, at]
            query = cut(rf, j) * fade_ref[d, 1, :, at]
            edge_row = tokens - 1 if d == 0 else 0
            last = fade_ref[d, 1, edge_row : edge_row + 1, at]
            base = sums[2 * d * tokens : (2 * d + 1) * tokens]
            rhs = jnp.concatenate([ahead.astype(bf16), base.astype(bf16)], 1)
            place = 4 * j + 2 * d
            solved = -dot(jnp.concatenate(inverses[place : place + 2], 1), rows_for_heads(rhs))
            solved = solved.astype(bf16)
            tail = fade_ref[d, 2, :, at]
            remove_tail = (units[j] * tail).astype(bf16)
            write_tail = (cut(kf, j) * tail).astype(bf16)
            seen = dot(jnp.concatenate(way["read"], 1), rows_for_heads(solved))
            query_ref[d, :, pair * LANES : (pair + 1) * LANES] = (query + cut(seen, 0)).astype(bf16)
            local = local + cut(seen, 1)
            onto = dot_cols(remove_tail, solved)
            transfer = jnp.where(block_diag, cut(onto, 0), 0.0) + eye * last
            transfer_ref[d, pair] = transfer.astype(bf16)
            carried = cut(onto, 1) + dot_cols(write_tail, vj)
            carried_ref[d, pair] = jnp.where(
                head0[:HEAD], carried[:HEAD], carried[HEAD:]
            )
        local_ref[:, pair * LANES : (pair + 1) * LANES] = local


def layer_kernel(
    nsp,
    nfs,
    ntp,
    x_hbm,
    in_gain_hbm,
    wk_hbm,
    wr_hbm,
    wv_hbm,
    wi_hbm,
    dl_hbm,
    rl_hbm,
    draise_hbm,
    dbias_hbm,
    rraise_hbm,
    rbias_hbm,
    tempo_hbm,
    extra_hbm,
    mix_hbm,
    gain_hbm,
    wa_hbm,
    wp_hbm,
    out_hbm,
    x_ref,
    in_gain_ref,
    draise_ref,
    dbias_ref,
    rraise_ref,
    rbias_ref,
    tempo_ref,
    extra_ref,
    gain_ref,
    wk_ref,
    wr_ref,
    wv_ref,
    wi_ref,
    dl_ref,
    rl_ref,
    mix_ref,
    wa_ref,
    wp_ref,
    loaded,
    mine,
    cells,
    part,
    pool_part,
    own_part,
    onward,
    pool_onward,
    landed,
    pool_landed,
    joined,
    pool_joined,
    xs,
    xr,
    ready,
    pr,
    qr,
    lat_ref,
    fade_ref,
    grow_ref,
    pool_ref,
    query_ref,
    local_ref,
    transfer_ref,
    carried_ref,
    edge,
    halo,
    rims,
    incoming,
    leaving,
    near_state,
    near_map,
    skipped,
    onto_next,
    act,
    tsend,
    trecv,
    sums_ref,
    osend,
    hs,
    hr,
    ss,
    sr,
    gr,
    ts,
    tr,
    os,
    orr,
):
    z = lax.axis_index("sp")
    me = lax.axis_index("fs")
    core = lax.axis_index("tp")
    tokens, channels = local_ref.shape
    depth = wa_ref.shape[0]
    half_rows = tokens // ntp
    has_prev = z > 0
    has_next = z < nsp - 1
    prev = jnp.maximum(z - 1, 0)
    after = jnp.minimum(z + 1, nsp - 1)
    prev2 = jnp.maximum(z - 2, 0)
    after2 = jnp.minimum(z + 2, nsp - 1)

    barrier = pltpu.get_barrier_semaphore()
    lead = core == ntp - 1

    @pl.when(lead)
    def _():
        for d in range(1, nfs):
            greet(barrier, "fs", flipped(me, d))

    @pl.when(jnp.logical_not(lead))
    def _():
        greet(barrier, "tp", ntp - 1)

    near = ((has_prev, prev), (has_next, after), (z > 1, prev2), (z < nsp - 2, after2))

    def greet_line():
        @pl.when(core == 0)
        def _():
            for there, peer in near:
                pl.when(there)(lambda: greet(barrier, "sp", peer))

    def meet_line():
        @pl.when(core == 0)
        def _():
            count = 0
            for there, _ in near:
                count = count + jnp.where(there, 1, 0)
            pl.semaphore_wait(barrier, count)
            for e in range(1, ntp):
                greet(ready, "tp", e)

        @pl.when(core != 0)
        def _():
            pl.semaphore_wait(ready, 1)

    small = (draise_hbm, dbias_hbm, rraise_hbm, rbias_hbm, tempo_hbm, extra_hbm, gain_hbm)
    sources = (x_hbm, in_gain_hbm, dl_hbm, rl_hbm, wk_hbm, wr_hbm, wv_hbm, wi_hbm)
    sources += small + (mix_hbm, wa_hbm, wp_hbm)
    small = (draise_ref, dbias_ref, rraise_ref, rbias_ref, tempo_ref, extra_ref, gain_ref)
    targets = (x_ref, in_gain_ref, dl_ref, rl_ref, wk_ref, wr_ref, wv_ref, wi_ref)
    targets += small + (mix_ref, wa_ref, wp_ref)
    loads = [
        pltpu.make_async_copy(source, target, loaded.at[i])
        for i, (source, target) in enumerate(zip(sources, targets))
    ]
    for load in loads:
        load.start()
    plan = group_plan(transfer_ref.shape[1])
    groups = len(plan)

    STATE, NEAR, MAP, SKIP = range(4)
    places = (z, nsp - 1 - z)
    odd = [lax.rem(place, 2) == 1 for place in places]

    def both(*tests):
        result = tests[0]
        for test in tests[1:]:
            result = jnp.logical_and(result, test)
        return result

    def state_copy(kind, d, g):
        span = pl.ds(plan[g][0], plan[g][1])
        source = (onto_next, leaving, transfer_ref, onto_next)[kind]
        target = (incoming, near_state, near_map, skipped)[kind]
        step = (after, prev) if kind != SKIP else (after2, prev2)
        return remote(
            source.at[d, span],
            target.at[d, span],
            ss.at[(0, 0, 1, 1)[kind], d, g],
            sr.at[(0, 0, 1, 2)[kind], d, g],
            "sp",
            step[d],
        )

    def starts(d):
        place = places[d]
        goes = place < nsp - 1
        return (
            (STATE, both(odd[d], goes)),
            (NEAR, both(jnp.logical_not(odd[d]), goes)),
            (MAP, both(jnp.logical_not(odd[d]), goes, place > 0)),
            (SKIP, both(odd[d], place < nsp - 2)),
        )

    ends = (pl.ds(tokens - HALO, HALO), pl.ds(0, HALO))

    def rim_copy(c, d, source, owner):
        return pltpu.make_async_remote_copy(
            src_ref=source,
            dst_ref=rims.at[d, c],
            send_sem=hs.at[c, d],
            recv_sem=hr.at[c, d],
            device_id={"fs": owner, "sp": after if d == 0 else prev},
            device_id_type=pl.DeviceIdType.MESH,
        )

    def send_rims(c, source, owner):
        for d in range(2):
            pl.when(sends[d])(lambda: rim_copy(c, d, source.at[ends[d]], owner).start())

    def own_rims(rows_of):
        for d in range(2):
            edge[d] = rows_of(ends[d]).astype(bf16)
            pl.when(sends[d])(lambda: rim_copy(0, d, edge.at[d], me).start())

    sends = [has_next, has_prev]
    takes = [has_prev, has_next]

    def pairs_of(g):
        return range(plan[g][0], plan[g][0] + plan[g][1])

    def mix_step(g, *operands):
        mix_group(plan[g][0], *operands)
        for d in range(2):

            @pl.when(places[d] == 0)
            def _():
                for p in pairs_of(g):
                    incoming[d, p] = jnp.zeros_like(incoming[d, p])

            for p in pairs_of(g):
                leaving[d, p] = carried_ref[d, p].astype(bf16)
            for kind, goes in starts(d)[NEAR : MAP + 1]:
                pl.when(goes)(lambda: state_copy(kind, d, g).start())

    def doubled(state):
        top0 = lax.broadcasted_iota(jnp.int32, state.shape, 1) < HEAD
        state = state.astype(f32)
        return jnp.concatenate([jnp.where(top0, state, 0.0), jnp.where(top0, 0.0, state)], 0)

    def moved(by, state):
        both_halves = dot(by, doubled(state))
        return both_halves[:HEAD] + both_halves[HEAD:]

    def relay(d, g):
        place = places[d]

        @pl.when(odd[d])
        def _():
            state_copy(NEAR, d, g).wait_recv()

            @pl.when(place == 1)
            def _():
                for p in pairs_of(g):
                    incoming[d, p] = near_state[d, p]

            @pl.when(place > 1)
            def _():
                state_copy(MAP, d, g).wait_recv()
                state_copy(SKIP, d, g).wait_recv()
                for p in pairs_of(g):
                    incoming[d, p] = (
                        moved(near_map[d, p], skipped[d, p]) + near_state[d, p].astype(f32)
                    ).astype(bf16)

            @pl.when(place < nsp - 1)
            def _():
                for p in pairs_of(g):
                    onto_next[d, p] = (
                        moved(transfer_ref[d, p], incoming[d, p]) + carried_ref[d, p]
                    ).astype(bf16)
                state_copy(STATE, d, g).start()
                pl.when(place < nsp - 2)(lambda: state_copy(SKIP, d, g).start())

        @pl.when(both(jnp.logical_not(odd[d]), place > 0))
        def _():
            state_copy(STATE, d, g).wait_recv()

    early = 2 * z < nsp

    def relays(near, g):
        @pl.when(early)
        def _():
            relay(0 if near else 1, g)

        @pl.when(jnp.logical_not(early))
        def _():
            relay(1 if near else 0, g)

    free_sends, settle_pool, finish_front = front_part(
        nfs,
        x_ref,
        in_gain_ref,
        (wk_ref, wr_ref, wv_ref, wi_ref),
        (dl_ref, rl_ref),
        loads[:15],
        pool_ref,
        lat_ref,
        mine,
        cells,
        part,
        pool_part,
        own_part,
        onward,
        pool_onward,
        landed,
        pool_landed,
        joined,
        pool_joined,
        xs,
        xr,
        loaded,
        pr,
        qr,
        nfs + ntp - 2,
        greet_line,
        meet_line,
        send_rims,
        own_rims,
        lambda: relays(True, 0),
        lambda g: prepare_group(
            plan[g][0],
            plan[g][1],
            lat_ref,
            draise_ref,
            dbias_ref,
            rraise_ref,
            rbias_ref,
            tempo_ref,
            extra_ref,
            fade_ref,
            grow_ref,
        ),
        lambda g, key, receptance, value: mix_step(
            g,
            key,
            receptance,
            value,
            fade_ref,
            grow_ref,
            query_ref,
            local_ref,
            transfer_ref,
            carried_ref,
        ),
    )
    for load in loads[15:]:
        load.wait()
    first, second, across = routes(me, nfs, core)

    def act_part(seq, k):
        if k == 0:
            return act.at[seq, 0]
        at, count = plan[k - 1]
        return act.at[seq, 1, :, pl.ds(at * LANES, count * LANES)]

    def share(k, seq, way, peer):
        return remote(
            act_part(seq, k), act_part(seq, k), loaded.at[3 * k + way], gr.at[k, way], "fs", peer
        )

    whole_way = groups

    def share_out(k):
        if k == whole_way:
            share(k, me, 2, across).start()
        share(k, me, 0, first).start()
        share(k, me, 1, second).start()

    def pass_on(k):
        share(k, first, 0, first).wait_recv()
        if k != whole_way:
            share(k, first, 2, second).start()

    head0 = lax.broadcasted_iota(jnp.int32, (tokens, LANES), 1) < HEAD

    def head_mean(values):
        low = jnp.sum(jnp.where(head0, values, 0.0), axis=-1, keepdims=True)
        high = jnp.sum(jnp.where(head0, 0.0, values), axis=-1, keepdims=True)
        return jnp.where(head0, low, high) * (1.0 / HEAD)

    def finish_group(g):
        with jax.named_scope(f"relayB{g}"):
            relays(False, g)
        with jax.named_scope(f"readout{g}"):
            for p in pairs_of(g):
                lanes = slice(p * LANES, (p + 1) * LANES)
                readout = local_ref[:, lanes]
                for d in range(2):
                    readout = readout + dot(query_ref[d, :, lanes], doubled(incoming[d, p]))
                centred = readout - head_mean(readout)
                scaled = centred * lax.rsqrt(head_mean(centred * centred) + head_eps)
                act[me, 1, :, lanes] = (
                    scaled * gain_ref[lanes].astype(f32).reshape(1, -1)
                ).astype(bf16)
            share_out(1 + g)

    for g in range(1, groups - 1):
        with jax.named_scope(f"relayA{g}"):
            relays(True, g)
    finish_group(0)
    free_sends()
    settle_pool()
    with jax.named_scope("halo"):
        for d in range(2):

            @pl.when(takes[d])
            def _():
                for c in range(3):
                    rim_copy(c, d, edge.at[d], me).wait_recv()
                halo[d] = sum(rims[d, c].astype(f32) for c in range(3)).astype(bf16)

            @pl.when(jnp.logical_not(takes[d]))
            def _():
                halo[d] = jnp.zeros_like(halo[d])

    span = tokens + 2 * HALO
    rim = jnp.concatenate([halo[0], pool_ref[...], halo[1]], 0)
    here = lax.broadcasted_iota(jnp.int32, (tokens, span), 0)
    there = lax.broadcasted_iota(jnp.int32, (tokens, span), 1) - HALO
    position = z * tokens + lax.broadcasted_iota(jnp.int32, (tokens, GROUP_WIDTH), 0)
    length = tokens * nsp
    groups_here = channels // GROUP_WIDTH
    for member in range(groups_here):
        cols = slice(member * GROUP_WIDTH, (member + 1) * GROUP_WIDTH)
        reach = jnp.left_shift(1, core * groups_here + member)
        window = jnp.where((there >= here - reach) & (there < here + reach), 1.0, 0.0)
        total = dot(window, rim[:, cols])
        size = (
            jnp.minimum(position + reach, length) - jnp.maximum(position - reach, 0)
        ).astype(f32)
        diff = (total / size - pool_ref[:, cols].astype(f32)).astype(bf16)
        act[me, 0, :, cols] = dot(diff, mix_ref[member]).astype(bf16)
    share_out(0)

    with jax.named_scope("relayAlast"):
        relays(True, groups - 1)
    for g in range(1, groups - 1):
        finish_group(g)
    finish_group(groups - 1)

    other = lax.rem(core + 1, ntp)
    mine_at = pl.multiple_of(core * half_rows, half_rows)
    other_at = pl.multiple_of(other * half_rows, half_rows)

    def product(seq, k):
        if k == 0:
            return dot_rows(act[seq, 0], wp_ref[...])
        at, count = plan[k - 1]
        cols = slice(at * LANES, (at + count) * LANES)
        return dot_rows(act[seq, 1, :, cols], wa_ref[:, cols])

    def swap_of(i):
        return remote(tsend.at[i], trecv.at[i], ts.at[i], tr.at[i], "tp", other)

    def offer(i, total):
        sums_ref[i] = total
        tsend[i] = sums_ref[i, pl.ds(other_at, half_rows)].astype(bf16)
        swap_of(i).start()

    place = out_hbm.at[0, :, pl.ds(pl.multiple_of(me * depth, depth), depth)]

    def back(i, seq):
        return remote(osend.at[i], place, os.at[i], orr.at[i], "fs", seq)

    own_out = pltpu.make_async_copy(osend.at[0], place, os.at[0])

    def settle_out(i, seq):
        swap_of(i).wait_recv()
        osend[i] = (
            sums_ref[i, pl.ds(mine_at, half_rows)] + trecv[i].astype(f32)
        ).astype(bf16)
        (back(i, seq) if i else own_out).start()

    with jax.named_scope("prodown"):
        offer(0, sum(product(me, k) for k in range(1 + groups)))
    peers = ((1, flipped(me, 1)), (2, flipped(me, nfs // 2)), (3, across))
    turn = list(range(groups))
    for k in turn:
        with jax.named_scope(f"pass{k}"):
            pass_on(k)
            share(k, second, 1, second).wait_recv()
        with jax.named_scope(f"prod{k}"):
            for i, seq in peers[:2]:
                sums_ref[i] = product(seq, k) + (sums_ref[i] if k != turn[0] else 0.0)
        if k == turn[0]:
            settle_out(0, me)
    k = groups
    with jax.named_scope(f"wait{k}1"):
        share(k, first, 0, first).wait_recv()
        share(k, second, 1, second).wait_recv()
    for i, seq in peers[:2]:
        with jax.named_scope(f"prod{k}{i}"):
            offer(i, product(seq, k) + sums_ref[i])
    for k in turn + [groups]:
        with jax.named_scope(f"wait{k}3"):
            share(k, across, 2, across).wait_recv()
        with jax.named_scope(f"prod{k}3"):
            total = product(across, k) + (sums_ref[3] if k != turn[0] else 0.0)
            if k < groups:
                sums_ref[3] = total
            else:
                offer(3, total)
        if k == turn[0]:
            for i, seq in peers[:2]:
                with jax.named_scope(f"swapwait{i}"):
                    settle_out(i, seq)
    with jax.named_scope("swapwait3"):
        settle_out(3, across)
    with jax.named_scope("sent"):
        own_out.wait()
        for k in range(1 + groups):
            for way in range(3):
                share(k, me, way, first).wait_send()
        for i in range(1 + len(peers)):
            swap_of(i).wait_send()
        for i, seq in peers:
            back(i, seq).wait_send()
        for d in range(2):

            @pl.when(sends[d])
            def _():
                for c in range(3):
                    rim_copy(c, d, edge.at[d], me).wait_send()

            for kind, goes in starts(d):

                @pl.when(goes)
                def _():
                    for g in range(groups):
                        state_copy(kind, d, g).wait_send()
        finish_front()
    with jax.named_scope("retwait"):
        for i, seq in peers:
            back(i, seq).wait_recv()


def shards(
    inputs,
    input_norm_gain,
    receptance_matrix,
    key_matrix,
    value_matrix,
    pooling_input_weight,
    decay_lower_matrix,
    decay_raise_matrix,
    decay_offset_bias,
    removal_lower_matrix,
    removal_raise_matrix,
    removal_rate_bias,
    tempo_scale,
    sudden_decay_extra,
    head_norm_gain,
    group_mixing_weight,
    attention_output_matrix,
    pooling_output_matrix,
):
    nsp, nfs, ntp = lax.axis_size("sp"), lax.axis_size("fs"), lax.axis_size("tp")
    _, tokens, features = inputs.shape
    depth, channels = key_matrix.shape
    pairs = channels // LANES
    groups = len(group_plan(pairs))
    dma = pltpu.SemaphoreType.DMA
    rank = decay_lower_matrix.shape[1]
    rank2 = decay_raise_matrix.shape[0] * decay_raise_matrix.shape[1]
    anywhere = pl.BlockSpec(memory_space=pl.ANY)
    half = (nfs, tokens // ntp, depth)
    return pl.pallas_call(
        functools.partial(layer_kernel, nsp, nfs, ntp),
        out_shape=pltpu.VMEM((1, tokens // ntp, features), bf16),
        in_specs=[anywhere] * 18,
        out_specs=anywhere,
        scratch_shapes=[
            pltpu.VMEM(inputs.shape, bf16),
            pltpu.VMEM(input_norm_gain.shape, bf16),
            pltpu.VMEM((rank2, channels), bf16),
            pltpu.VMEM(decay_offset_bias.shape, f32),
            pltpu.VMEM((rank2, channels), bf16),
            pltpu.VMEM(removal_rate_bias.shape, f32),
            pltpu.VMEM(tempo_scale.shape[1:], f32),
            pltpu.VMEM(sudden_decay_extra.shape[1:], f32),
            pltpu.VMEM(head_norm_gain.shape, bf16),
        ]
        + [pltpu.VMEM((depth, channels), bf16)] * 4
        + [
            pltpu.VMEM((features, rank), bf16),
            pltpu.VMEM((features, rank), bf16),
            pltpu.VMEM(group_mixing_weight.shape, bf16),
            pltpu.VMEM(attention_output_matrix.shape, bf16),
            pltpu.VMEM(pooling_output_matrix.shape, bf16),
            dma((18,)),
            pltpu.VMEM((nfs, tokens, depth), bf16),
            pltpu.VMEM((nfs, tokens, depth), bf16),
            pltpu.VMEM((2, pairs, 3, tokens, LANES), bf16),
            pltpu.VMEM((2, tokens, channels), bf16),
            pltpu.VMEM((pairs, 3, tokens, LANES), f32),
            pltpu.VMEM((pairs, 3, tokens, LANES), bf16),
            pltpu.VMEM((tokens, channels), bf16),
            pltpu.VMEM((2, pairs, 3, tokens, LANES), bf16),
            pltpu.VMEM((2, tokens, channels), bf16),
            pltpu.VMEM((pairs, 3, tokens, LANES), bf16),
            pltpu.VMEM((tokens, channels), bf16),
            dma((nfs - 1, ntp)),
            dma((nfs - 1,)),
            pltpu.SemaphoreType.REGULAR,
            dma((groups + 1, 2)),
            dma((groups + 1,)),
            pltpu.VMEM((2, tokens, rank), bf16),
            pltpu.VMEM((2, 5, tokens, channels), f32),
            pltpu.VMEM((2, tokens // BLOCK, tokens, channels), f32),
            pltpu.VMEM((tokens, channels), bf16),
            pltpu.VMEM((2, tokens, channels), bf16),
            pltpu.VMEM((tokens, channels), f32),
            pltpu.VMEM((2, pairs, LANES, LANES), bf16),
            pltpu.VMEM((2, pairs, HEAD, LANES), f32),
            pltpu.VMEM((2, HALO, channels), bf16),
            pltpu.VMEM((2, HALO, channels), bf16),
            pltpu.VMEM((2, 3, HALO, channels), bf16),
            pltpu.VMEM((2, pairs, HEAD, LANES), bf16),
            pltpu.VMEM((2, pairs, HEAD, LANES), bf16),
            pltpu.VMEM((2, pairs, HEAD, LANES), bf16),
            pltpu.VMEM((2, pairs, LANES, LANES), bf16),
            pltpu.VMEM((2, pairs, HEAD, LANES), bf16),
            pltpu.VMEM((2, pairs, HEAD, LANES), bf16),
            pltpu.VMEM((nfs, 2, tokens, channels), bf16),
            pltpu.VMEM(half, bf16),
            pltpu.VMEM(half, bf16),
            pltpu.VMEM((nfs, tokens, depth), f32),
            pltpu.VMEM(half, bf16),
            dma((3, 2)),
            dma((3, 2)),
            dma((2, 2, groups)),
            dma((3, 2, groups)),
            dma((1 + groups, 3)),
            dma((nfs,)),
            dma((nfs,)),
            dma((nfs,)),
            dma((nfs,)),
        ],
        compiler_params=pltpu.CompilerParams(
            collective_id=0, has_side_effects=True, vmem_limit_bytes=60 * 1024 * 1024
        ),
        name="layer",
    )(
        inputs,
        input_norm_gain,
        key_matrix,
        receptance_matrix,
        value_matrix,
        pooling_input_weight,
        decay_lower_matrix,
        removal_lower_matrix,
        decay_raise_matrix.reshape(rank2, channels),
        decay_offset_bias,
        removal_raise_matrix.reshape(rank2, channels),
        removal_rate_bias,
        tempo_scale[0],
        sudden_decay_extra[0],
        group_mixing_weight,
        head_norm_gain,
        attention_output_matrix,
        pooling_output_matrix,
    )


def solution(mesh):
    in_specs = (
        P("fs", "sp", None),
        P(),
        P("fs", "tp"),
        P("fs", "tp"),
        P("fs", "tp"),
        P("fs", "tp"),
        P(),
        P(None, None, "tp"),
        P(None, "tp"),
        P(),
        P(None, None, "tp"),
        P(None, "tp"),
        P("fs", None, "tp", "sp"),
        P("fs", None, "tp", "sp"),
        P("tp"),
        P("tp", None, None),
        P("fs", "tp"),
        P("fs", "tp"),
    )
    out_specs = P("fs", ("sp", "tp"), None)
    return jax.shard_map(shards, mesh=mesh, in_specs=in_specs, out_specs=out_specs, check_vma=False)
```
